512 devices in a mesh: sp: 32 (over z, x), tp: 16 (over y, core).
Axes of the slice: x: 4, y: 8, z: 8, core: 2. Of those that a mesh axis runs over, the one named last changes fastest.
Arguments:
- lane_source_signal: bfloat16 [1024, 4096], P('tp', 'sp'), may hold values from -6 to 6
- spectral_damping_part: float32 [64, 64], P('tp'), may hold values from -3 to -0.0002
- spectral_angular_part: float32 [64, 64], P('tp'), may hold values from 0.31 to 201.0624
- interval_exponent: float32 [64], P('tp'), may hold values from -3.9 to -1.6
- entry_matrix_inphase: float32 [64, 64, 16], P('tp'), may hold values from -1 to 1
- entry_matrix_quadrature: float32 [64, 64, 16], P('tp'), may hold values from -1 to 1
- emission_inphase: float32 [64, 16, 64], P('tp'), may hold values from -0.75 to 0.75
- emission_quadrature: float32 [64, 16, 64], P('tp'), may hold values from -0.75 to 0.75
- lane_bypass_factor: float32 [1024], P('tp'), may hold values from -5 to 5
- spike_shrink_offset: float32 [64, 4096], P('tp', 'sp'), may hold values from -1.4 to 0
- lane_exit_matrix: bfloat16 [1024, 4096], P('tp'), may hold values from -0.1875 to 0.1875
- skipline_stream: bfloat16 [4096, 4096], P('sp'), may hold values from -6 to 6
- specialist_scaling_vector: float32 [4096], replicated, may hold values from 0.1 to 1.9
- selected_specialists: int32 [4096, 2], P('sp'), may hold values from 0 to 31, all different within a row; in each aligned block of 128 rows (0 to 127, 128 to 255, ...) at most 16 rows name the same one
- dispatcher_scores: float32 [4096, 2], P('sp'), may hold values from 0.1 to 1
- specialist_valve_matrix: bfloat16 [32, 4096, 2048], P('sp', None, 'tp'), may hold values from -0.09375 to 0.09375
- specialist_widen_matrix: bfloat16 [32, 4096, 2048], P('sp', None, 'tp'), may hold values from -0.09375 to 0.09375
- specialist_shrink_matrix: bfloat16 [32, 2048, 4096], P('sp', 'tp'), may hold values from -0.1875 to 0.1875
Outputs:
- updated: bfloat16 [4096, 4096], P('sp', 'tp')
The draws below stay inside these ranges and needn't reach their ends.
Inputs may be any that keep to these rules, and one draw needn't show every extreme that they name: `selected_specialists`: each row names 2 different experts. Among the rows of each aligned block of 128 positions no expert is named more than 16 times, and in every block some expert is named exactly 16 times.
All inputs are finite; a program needn't handle non-finite values.
Results may differ from the reference program's by a relative error of at most 0.019.
Values may be sent and summed in bfloat16 or wider, within the bound.
A program may use at most 64 MiB of HBM per device.

```python
import math
import jax
import jax.numpy as jnp
import numpy as np
from jax import lax

D = 4096
C = 1024
GS = 16
P_SIZE = 64
F = 2048
TOPK = 2
TOK_DEV = 128
G = 64
TOKENS = 4096
EXPERTS = 32
CAP = 16
N_SP = 32
N_TP = 16


def draw_spectral_damping_part(key, part):
    subkeys = jax.random.split(key, 3)
    fast_group = jax.random.uniform(subkeys[0], (G, 1)) < 0.5
    quick_rate = -jax.random.uniform(subkeys[1], (G, P_SIZE), jnp.float32, 1.0, 3.0)
    slow_rate = -jnp.exp(jax.random.uniform(subkeys[2], (G, P_SIZE), jnp.float32, math.log(0.0002), math.log(0.001)))
    return jnp.where(fast_group, quick_rate, slow_rate)


def draw_spectral_angular_part(key, part):
    offset = jax.random.uniform(key, (G, P_SIZE), jnp.float32, 0.1, 0.9)
    return math.pi * (jnp.arange(P_SIZE, dtype=jnp.float32)[None, :] + offset)


def draw_spike_shrink_offset(key, part):
    subkeys = jax.random.split(key, 3)
    blocks = TOKENS // 32
    block_rate = jnp.exp(jax.random.uniform(subkeys[0], (G, blocks), jnp.float32, math.log(2.5e-05), math.log(0.0001)))
    baseline = -jnp.repeat(block_rate, 32, axis=1)
    spots = jax.random.randint(subkeys[1], (G, 2), 0, TOKENS)
    losses = jnp.log(1.0 - jax.random.uniform(subkeys[2], (G, 2), jnp.float32, 0.2, 0.5))
    position = jnp.arange(TOKENS, dtype=jnp.int32)[None, :, None]
    struck = position == spots[:, None, :]
    return baseline + jnp.sum(jnp.where(struck, losses[:, None, :], 0.0), axis=2)


def raised(result, stream_key, source, target, shards_of, factor):
    owner, partner = [(jnp.arange(result.shape[dim]) // (result.shape[dim] // shards_of)).reshape([-1 if axis == dim else 1 for axis in range(result.ndim)]) for dim in (source, target)]
    chosen = jax.random.permutation(stream_key, shards_of)[partner]
    strong = (owner == chosen) | (owner == (partner + shards_of // 2) % shards_of)
    return jnp.where(strong, factor * result, result)


def steps_of(stream_key, shape, cuts, smallest, top_value):
    def one(dim, shards_of):
        steps = jax.random.uniform(jax.random.fold_in(jax.random.fold_in(stream_key, 6), dim), (shards_of,), jnp.float32, smallest / len(cuts), top_value / len(cuts))
        return jnp.repeat(jnp.exp(steps), shape[dim] // shards_of).reshape((-1,) + (1,) * (len(shape) - dim - 1))

    factor_of = one(*cuts[0])
    for cut in cuts[1:]:
        factor_of = factor_of * one(*cut)
    return factor_of


def assign_block(rng, own, number, rows, number_of, top, most, skew):
    sequence = jax.random.permutation(rng, number_of)
    crowded, common = shares(number_of, rows * top, most, skew, True), shares(number_of, rows * top, most, skew, False)
    places = jnp.arange(number_of)

    def named(tallies, turn):
        used = int((tallies > 0).sum())
        fixed = max(1, used // 4)
        moved = fixed + (places - fixed + turn * (used - fixed)) % max(1, number_of - fixed)
        return jnp.zeros((number_of,), jnp.int32).at[sequence[jnp.where(places < fixed, places, moved)]].set(jnp.asarray(tallies, jnp.int32))

    tallies = jnp.where(number % 4 == 0, named(crowded, number // 4), named(common, number - number // 4 - 1))
    mixed = jax.random.permutation(jax.random.fold_in(own, 3), number_of)
    giver, sink = mixed[0:number_of // 2 * 2:2], mixed[1:number_of // 2 * 2:2]
    slack = jnp.minimum(tallies[giver] - 1, most - tallies[sink]) // 2
    slack = jnp.where((giver == sequence[0]) | (sink == sequence[0]) | (tallies[sink] == 0), 0, jnp.maximum(slack, 0))
    moved = jax.random.randint(jax.random.fold_in(own, 4), (number_of // 2,), 0, 1 << 20) % (slack + 1)
    tallies = tallies.at[giver].add(-moved).at[sink].add(moved)
    members = jnp.searchsorted(jnp.cumsum(tallies), jnp.arange(rows * top), side="right").astype(jnp.int32)
    listing = members.reshape(top, rows).T
    listing = listing[jax.random.permutation(jax.random.fold_in(own, 1), rows)]
    turn = jax.random.randint(jax.random.fold_in(own, 2), (rows, 1), 0, top)
    return jnp.take_along_axis(listing, (jnp.arange(top)[None, :] + turn) % top, axis=1)


def shares(number_of, total, reach, lean, full):
    loads = [(1 << 20) // math.isqrt(grade ** lean) + 1 for grade in range(1, number_of + 1)]
    largest = reach if full else min(reach, max(-(-total // number_of), total * loads[0] // sum(loads)))
    least = 1 if total - largest >= number_of - 1 else 0
    given, surplus = [largest] + [least] * (number_of - 1), total - largest - least * (number_of - 1)
    while surplus > 0:
        free = [i for i in range(1, number_of) if given[i] < largest] or [i for i in range(1, number_of) if given[i] < reach]
        whole, left = sum([loads[i] for i in free]), surplus
        for i in free:
            more = min(reach - given[i], max(1, left * loads[i] // whole), surplus)
            given[i] = given[i] + more
            surplus = surplus - more
    return np.array(given)


def centred(key, shape, width, most, pieces=(), kind=jnp.bfloat16):
    gain = steps_of(key, shape, pieces, -0.22, 0.18) if pieces else 1.0
    result = jax.random.normal(key, shape, jnp.float32) * width * gain
    return jnp.minimum(jnp.maximum(result, -most), most).astype(kind)


def heavy_noise(own_key, extent, width, most, shards, heavy, kind=jnp.bfloat16):
    array = width * jax.random.normal(own_key, extent, jnp.float32)
    if shards:
        array = array * steps_of(own_key, extent, shards, -0.22, 0.18)
    return jnp.clip(raised(array, jax.random.fold_in(own_key, 3), *heavy), -most, most).astype(kind)


def setup_inputs(seed: int = 0) -> dict:
    streams_of = jax.random.split(jax.random.key(seed), 19)
    lane_source_signal = centred(streams_of[0], (C, TOKENS), 1.0, 6.0, ((0, 16), (1, 32)))
    spectral_damping_part = draw_spectral_damping_part(jax.random.fold_in(streams_of[18], 71), 0)
    spectral_angular_part = draw_spectral_angular_part(jax.random.fold_in(streams_of[18], 71), 0)
    interval_exponent = jnp.clip(-3.9 + 2.3000001 * jax.random.uniform(streams_of[3], (G,), jnp.float32) ** steps_of(streams_of[3], (G,), ((0, 16),), -0.2, 0.2), -3.9, -1.6)
    entry_matrix_inphase = centred(streams_of[4], (G, P_SIZE, GS), (2 * GS) ** -0.5, 1.0, ((0, 16),), jnp.float32)
    entry_matrix_quadrature = centred(streams_of[5], (G, P_SIZE, GS), (2 * GS) ** -0.5, 1.0, ((0, 16),), jnp.float32)
    emission_inphase = centred(streams_of[6], (G, GS, P_SIZE), P_SIZE ** -0.5, 0.75, ((0, 16),), jnp.float32)
    emission_quadrature = centred(streams_of[7], (G, GS, P_SIZE), P_SIZE ** -0.5, 0.75, ((0, 16),), jnp.float32)
    lane_bypass_factor = centred(streams_of[8], (C,), 1.0, 5.0, ((0, 16),), jnp.float32)
    spike_shrink_offset = draw_spike_shrink_offset(jax.random.fold_in(streams_of[18], 71), 0)
    lane_exit_matrix = centred(streams_of[10], (C, D), C ** -0.5, 0.1875, ((0, 16),))
    skipline_stream = centred(streams_of[11], (TOKENS, D), 1.0, 6.0, ((0, 32),))
    specialist_scaling_vector = jnp.clip(1.0 + 0.18 * jax.random.normal(streams_of[12], (D,), jnp.float32), 0.1, 1.9)
    selected_specialists_keys = jax.random.split(jax.random.fold_in(streams_of[13], 1), TOKENS // TOK_DEV)
    selected_specialists_turns = jax.random.permutation(jax.random.fold_in(streams_of[13], 3), TOKENS // TOK_DEV)
    selected_specialists = jax.vmap(lambda own, number: assign_block(jax.random.fold_in(streams_of[13], 2), own, number, TOK_DEV, EXPERTS, TOPK, CAP, 2))(selected_specialists_keys, selected_specialists_turns).reshape((TOKENS, TOPK))
    dispatcher_scores = jnp.clip(jnp.exp(math.log(1.0) - 2.3025851 * jax.random.uniform(streams_of[14], (TOKENS, TOPK), jnp.float32) ** steps_of(streams_of[14], (TOKENS, TOPK), ((0, 32),), -0.2, 0.2)), 0.1, 1.0)
    specialist_valve_matrix = centred(streams_of[15], (EXPERTS, D, F), D ** -0.5, 0.09375, ((0, 32), (2, 16)))
    specialist_widen_matrix = centred(streams_of[16], (EXPERTS, D, F), D ** -0.5, 0.09375, ((0, 32), (2, 16)))
    specialist_shrink_matrix = heavy_noise(streams_of[17], (EXPERTS, F, D), F ** -0.5, 0.1875, ((0, 32), (1, 16)), (1, 2, 16, 2.0))
    return {"lane_source_signal": lane_source_signal, "spectral_damping_part": spectral_damping_part, "spectral_angular_part": spectral_angular_part, "interval_exponent": interval_exponent, "entry_matrix_inphase": entry_matrix_inphase, "entry_matrix_quadrature": entry_matrix_quadrature, "emission_inphase": emission_inphase, "emission_quadrature": emission_quadrature, "lane_bypass_factor": lane_bypass_factor, "spike_shrink_offset": spike_shrink_offset, "lane_exit_matrix": lane_exit_matrix, "skipline_stream": skipline_stream, "specialist_scaling_vector": specialist_scaling_vector, "selected_specialists": selected_specialists, "dispatcher_scores": dispatcher_scores, "specialist_valve_matrix": specialist_valve_matrix, "specialist_widen_matrix": specialist_widen_matrix, "specialist_shrink_matrix": specialist_shrink_matrix}


EPS = 1e-06
PRECISE_MODE = lax.Precision.HIGHEST

def affine_pair(earlier, latter):
    mul_re = earlier[0] * latter[0] - earlier[1] * latter[1]
    mul_im = earlier[0] * latter[1] + earlier[1] * latter[0]
    add_re = latter[0] * earlier[2] - latter[1] * earlier[3] + latter[2]
    add_im = latter[0] * earlier[3] + latter[1] * earlier[2] + latter[3]
    return (mul_re, mul_im, add_re, add_im)

def bundled_recurrence_layer(packed):
    u_group, a_real, a_imag, log_dt, b_real, b_imag, c_real, c_imag, skip_group, extra_row = packed
    step_size = jnp.exp(log_dt)
    natural_pace_exponent = a_real * step_size
    angle = a_imag * step_size
    num_re = jnp.expm1(natural_pace_exponent) * jnp.cos(angle) - 2.0 * jnp.sin(0.5 * angle) ** 2
    num_im = jnp.exp(natural_pace_exponent) * jnp.sin(angle)
    denom = a_real * a_real + a_imag * a_imag
    fac_re = (num_re * a_real + num_im * a_imag) / denom
    fac_im = (num_im * a_real - num_re * a_imag) / denom
    map_re = fac_re[:, None] * b_real - fac_im[:, None] * b_imag
    map_im = fac_re[:, None] * b_imag + fac_im[:, None] * b_real
    drive_re = jnp.dot(map_re, u_group, precision=PRECISE_MODE)
    drive_im = jnp.dot(map_im, u_group, precision=PRECISE_MODE)
    recurrence_modulus = jnp.exp(natural_pace_exponent[:, None] + extra_row[None, :])
    trans_re = recurrence_modulus * jnp.cos(angle)[:, None]
    trans_im = recurrence_modulus * jnp.sin(angle)[:, None]
    scanned = lax.associative_scan(affine_pair, (trans_re, trans_im, drive_re, drive_im), axis=1)
    value = jnp.dot(c_real, scanned[2], precision=PRECISE_MODE) - jnp.dot(c_imag, scanned[3], precision=PRECISE_MODE) + skip_group[:, None] * u_group
    return jax.nn.gelu(value).astype(jnp.bfloat16)

def reference(lane_source_signal, spectral_damping_part, spectral_angular_part, interval_exponent, entry_matrix_inphase, entry_matrix_quadrature, emission_inphase, emission_quadrature, lane_bypass_factor, spike_shrink_offset, lane_exit_matrix, skipline_stream, specialist_scaling_vector, selected_specialists, dispatcher_scores, specialist_valve_matrix, specialist_widen_matrix, specialist_shrink_matrix):
    f32 = jnp.float32
    bf16 = jnp.bfloat16
    bundle_total = spectral_damping_part.shape[0]
    lanes_within_bundle = entry_matrix_inphase.shape[2]
    length = lane_source_signal.shape[1]
    bundled_signal = lane_source_signal.astype(f32).reshape(bundle_total, lanes_within_bundle, length)
    recurrence_result = lax.map(bundled_recurrence_layer, (bundled_signal, spectral_damping_part, spectral_angular_part, interval_exponent, entry_matrix_inphase, entry_matrix_quadrature, emission_inphase, emission_quadrature, lane_bypass_factor.reshape(bundle_total, lanes_within_bundle), spike_shrink_offset))
    recurrence_result = recurrence_result.reshape(bundle_total * lanes_within_bundle, length)
    projected = jnp.dot(recurrence_result.T, lane_exit_matrix, preferred_element_type=f32).astype(bf16)
    stream = (skipline_stream.astype(f32) + lax.optimization_barrier(projected).astype(f32)).astype(bf16)
    stream_f = lax.optimization_barrier(stream).astype(f32)
    inv_rms = lax.rsqrt(lax.optimization_barrier(jnp.mean(stream_f * stream_f, axis=-1, keepdims=True)) + EPS)
    normed = (stream_f * inv_rms * specialist_scaling_vector).astype(bf16)
    share = dispatcher_scores / lax.optimization_barrier(jnp.sum(dispatcher_scores, axis=1, keepdims=True))
    flat_routes = selected_specialists.reshape(-1)
    flat_share = share.reshape(-1)
    slots = N_SP * CAP
    block_units = F // N_TP

    def one_expert(total, packed):
        gate_w, up_w, down_w, expert_id = packed
        chosen = flat_routes == expert_id
        positions = jnp.nonzero(chosen, size=slots, fill_value=0)[0].astype(jnp.int32)
        valid = jnp.arange(slots, dtype=jnp.int32) < jnp.sum(chosen.astype(jnp.int32))
        token_ids = positions // TOPK
        rows = normed[token_ids]
        gate_part = jnp.dot(rows, gate_w, preferred_element_type=f32)
        up_part = jnp.dot(rows, up_w, preferred_element_type=f32)
        hidden = (jax.nn.silu(gate_part) * up_part).astype(bf16)
        hidden_blocks = jnp.transpose(hidden.reshape(slots, N_TP, block_units), (1, 0, 2))
        down_blocks = down_w.reshape(N_TP, block_units, down_w.shape[1])

        def add_block(acc, pair):
            part = jnp.dot(pair[0], pair[1], preferred_element_type=f32).astype(bf16)
            return (acc + lax.optimization_barrier(part).astype(f32), None)
        acc0 = jnp.zeros((slots, down_w.shape[1]), f32)
        summed, _ = lax.scan(add_block, acc0, (hidden_blocks, down_blocks))
        expert_out = lax.optimization_barrier(summed.astype(bf16)).astype(f32)
        weights = jnp.where(valid, flat_share[positions], 0.0)
        return (total.at[token_ids].add(weights[:, None] * expert_out), None)
    start = jnp.zeros(stream_f.shape, f32)
    experts = specialist_valve_matrix.shape[0]
    moe, _ = lax.scan(one_expert, start, (specialist_valve_matrix, specialist_widen_matrix, specialist_shrink_matrix, jnp.arange(experts, dtype=jnp.int32)))
    return (stream_f + moe).astype(bf16)
```

```python
import functools

import jax
import jax.numpy as jnp
from jax import lax
from jax.experimental import pallas as pl
from jax.experimental.pallas import tpu as pltpu
from jax.sharding import PartitionSpec as P

EPS = 1e-06
HIGH = lax.Precision.HIGHEST
MESH = pl.DeviceIdType.MESH
F32 = jnp.float32
BF16 = jnp.bfloat16
CORES = 2
CHUNKS = 4
SKEW = 1


def iota(shape, dim):
    return lax.broadcasted_iota(jnp.int32, shape, dim)


def to_col(row):
    n = row.shape[1]
    eye = iota((n, n), 0) == iota((n, n), 1)
    return jnp.sum(jnp.where(eye, row, 0.0), axis=1, keepdims=True)


def to_row(col):
    n = col.shape[0]
    eye = iota((n, n), 0) == iota((n, n), 1)
    return jnp.sum(jnp.where(eye, col, 0.0), axis=0, keepdims=True)


def small_expm1(x):
    total = jnp.ones_like(x)
    for k in range(11, 1, -1):
        total = 1.0 + total * x * (1.0 / k)
    return jnp.where(x > -0.7, x * total, jnp.exp(x) - 1.0)


def times(ar, ai, br, bi):
    return ar * br - ai * bi, ar * bi + ai * br


def mixer_kernel(
    dims,
    u_ref, damp_ref, ang_ref, ie_ref, ein_ref, eq_ref, cin_ref, cq_ref, byp_ref, off_ref,
    sel_ref, score_ref, wexit_hbm, skip_hbm, gain_hbm, gate_hbm, up_hbm, down_hbm,
    out_ref,
    msg, heads, wx, mx, dw, gu, skip, gain, ss, inv, rinv, disp, whi, wlo,
    xs, g_buf, h_buf, acc, oacc, outb, ret, stream_s, loc_r, cum_r, cum_i,
    l_sem, s_pre, r_pre, s_wx, r_wx, s_mx, r_mx, s_dw, r_dw, s_ss, r_ss,
    s_inv, r_inv, s_dis, r_dis, s_ret, r_ret, s_g, r_g, s_h, r_h,
):
    n_sp, n_tp, groups, states, lanes, tok, width, cap = dims
    n_y = n_tp // CORES
    d_local = width // n_tp
    f_local = gate_hbm.shape[2]
    slots = n_sp * cap
    rows_q = slots // CHUNKS
    sp_q = n_sp // CHUNKS
    me, mt = lax.axis_index("sp"), lax.axis_index("tp")
    y, core = mt // CORES, mt % CORES
    twin = y * CORES + (1 - core)

    def each(count, mine, fn):
        def step(j, carry):
            fn(lax.rem(mine + j, count))
            return carry
        lax.fori_loop(1, count, step, 0)

    def span(lo, hi, fn):
        def step(j, carry):
            fn(j)
            return carry
        lax.fori_loop(lo, hi, step, 0)

    def remote(src, dst, send, recv, sp, tp):
        return pltpu.make_async_remote_copy(
            src_ref=src, dst_ref=dst, send_sem=send, recv_sem=recv,
            device_id=(sp, tp), device_id_type=MESH)

    heads[...] = jnp.zeros_like(heads)
    barrier = pltpu.get_barrier_semaphore()
    each(n_sp, me, lambda k: pl.semaphore_signal(
        barrier, inc=1, device_id=(k, mt), device_id_type=MESH))
    each(n_tp, mt, lambda k: pl.semaphore_signal(
        barrier, inc=1, device_id=(me, k), device_id_type=MESH))

    own_cols = pl.ds(pl.multiple_of(mt * d_local, d_local), d_local)
    chan = groups * lanes
    local = [
        pltpu.make_async_copy(skip_hbm.at[:, own_cols], skip, l_sem.at[0]),
        pltpu.make_async_copy(gain_hbm.at[:, own_cols], gain, l_sem.at[1]),
        pltpu.make_async_copy(wexit_hbm.at[:, own_cols], wx.at[mt], l_sem.at[2]),
        pltpu.make_async_copy(gate_hbm.at[0], gu.at[:, pl.ds(0, f_local)], l_sem.at[3]),
        pltpu.make_async_copy(up_hbm.at[0], gu.at[:, pl.ds(f_local, f_local)], l_sem.at[4]),
        pltpu.make_async_copy(down_hbm.at[0, :, own_cols], dw.at[mt], l_sem.at[5]),
    ]
    for copy in local:
        copy.start()

    step_size = jnp.exp(to_col(ie_ref[...]))
    damp, ang = damp_ref[...], ang_ref[...]
    rate, angle = damp * step_size, ang * step_size
    cos, sin = jnp.cos(angle), jnp.sin(angle)
    half = jnp.sin(0.5 * angle)
    num_re = small_expm1(rate) * cos - 2.0 * half * half
    num_im = jnp.exp(rate) * sin
    denom = damp * damp + ang * ang
    fac_re = (num_re * damp + num_im * ang) / denom
    fac_im = (num_im * damp - num_re * ang) / denom
    total = off_ref[...]
    lane_g = iota(total.shape, 1)
    shift = 1
    while shift < tok:
        total = total + jnp.where(lane_g >= shift, pltpu.roll(total, shift, 1), 0.0)
        shift *= 2
    lane = iota((states, tok), 1)
    bypass = byp_ref[...]
    for g in range(groups):
        row = slice(g, g + 1)
        u = u_ref[g * lanes:(g + 1) * lanes, :].astype(F32)
        e_re = jnp.dot(ein_ref[g], u, precision=HIGH, preferred_element_type=F32)
        e_im = jnp.dot(eq_ref[g], u, precision=HIGH, preferred_element_type=F32)
        f_re, f_im = to_col(fac_re[row]), to_col(fac_im[row])
        s_re, s_im = times(f_re, f_im, e_re, e_im)
        rate_c = to_col(rate[row])
        w_re, w_im = to_col(cos[row]), to_col(sin[row])
        sums = total[row]
        p_re, p_im = jnp.ones((states, tok), F32), jnp.zeros((states, tok), F32)
        shift = 1
        while shift <= tok:
            taken = (jnp.bitwise_and(lane + 1, shift)) != 0
            q_re, q_im = times(p_re, p_im, w_re, w_im)
            p_re, p_im = jnp.where(taken, q_re, p_re), jnp.where(taken, q_im, p_im)
            if shift < tok:
                gap = sums - pltpu.roll(sums, shift, 1)
                size = jnp.exp(rate_c * float(shift) + jnp.minimum(gap, 0.0))
                size = jnp.where(lane >= shift, size, 0.0)
                t_re, t_im = times(
                    w_re, w_im, pltpu.roll(s_re, shift, 1), pltpu.roll(s_im, shift, 1))
                s_re, s_im = s_re + size * t_re, s_im + size * t_im
                w_re, w_im = times(w_re, w_im, w_re, w_im)
            shift *= 2
        size = jnp.exp(rate_c * (lane + 1).astype(F32) + sums)
        cum_r[g], cum_i[g] = size * p_re, size * p_im
        last = lane == tok - 1
        h_re = to_row(jnp.sum(jnp.where(last, s_re, 0.0), axis=1, keepdims=True))
        h_im = to_row(jnp.sum(jnp.where(last, s_im, 0.0), axis=1, keepdims=True))
        end = jnp.sum(jnp.where(lane_g[row] == tok - 1, sums, 0.0), axis=1, keepdims=True)
        msg[g:g + 1, 0:states] = h_re
        msg[g:g + 1, states:2 * states] = jnp.broadcast_to(end, (1, states))
        msg[groups + g:groups + g + 1, 0:states] = h_im
        msg[groups + g:groups + g + 1, states:2 * states] = jnp.zeros((1, states), F32)
        loc_r[g] = (
            jnp.dot(cin_ref[g], s_re, precision=HIGH, preferred_element_type=F32)
            - jnp.dot(cq_ref[g], s_im, precision=HIGH, preferred_element_type=F32)
            + to_col(bypass[:, g * lanes:(g + 1) * lanes]) * u)

    pl.semaphore_wait(barrier, n_sp - 1 + n_tp - 1)

    def send_head(k):
        return remote(msg, heads.at[me], s_pre.at[k], r_pre.at[me], k, mt)

    def head_from(k):
        return remote(msg, heads.at[k], s_pre.at[k], r_pre.at[k], me, mt)

    span(me + 1, n_sp, lambda k: send_head(k).start())

    def columns_of(k):
        return pl.ds(pl.multiple_of(k * d_local, d_local), d_local)

    def send_wx(k):
        return remote(
            wexit_hbm.at[:, columns_of(k)], wx.at[mt], s_wx.at[k], r_wx.at[mt], me, k)

    def send_dw(k):
        return remote(
            down_hbm.at[0, :, columns_of(k)], dw.at[mt], s_dw.at[k], r_dw.at[mt], me, k)

    each(n_tp, mt, lambda k: send_wx(k).start())

    sel, score = sel_ref[...], score_ref[...]
    expert = iota((tok, n_sp), 1)
    hit0 = (sel[:, 0:1] == expert).astype(F32)
    hit1 = (sel[:, 1:2] == expert).astype(F32)
    hits = (hit0 + hit1).astype(BF16)
    below = (iota((tok, tok), 1) < iota((tok, tok), 0)).astype(F32).astype(BF16)
    rank = jnp.dot(below, hits, preferred_element_type=F32).astype(BF16)
    slot_e, slot_j = iota((n_sp, slots), 0), iota((n_sp, slots), 1)
    spread = ((slot_j >= slot_e * cap) & (slot_j < (slot_e + 1) * cap)).astype(F32).astype(BF16)
    hits_x = jnp.dot(hits, spread, preferred_element_type=F32)
    hit0_x = jnp.dot(hit0.astype(BF16), spread, preferred_element_type=F32)
    rank_x = jnp.dot(rank, spread, preferred_element_type=F32)
    place = jnp.bitwise_and(iota((tok, slots), 1), cap - 1).astype(F32)
    picked = (hits_x > 0.5) & (rank_x == place)
    disp[...] = picked.astype(F32).astype(BF16)
    both = score[:, 0:1] + score[:, 1:2]
    share = jnp.where(hit0_x > 0.5, score[:, 0:1] / both, score[:, 1:2] / both)
    share = jnp.where(picked, share, 0.0)
    high = share.astype(BF16)
    whi[...] = high
    wlo[...] = (share - high.astype(F32)).astype(BF16)

    span(0, me, lambda k: head_from(k).wait_recv())
    w_re, w_im = cos, sin
    shift = 1
    while shift < tok:
        w_re, w_im = times(w_re, w_im, w_re, w_im)
        shift *= 2
    in_re, in_im = jnp.zeros_like(rate), jnp.zeros_like(rate)
    for k in range(n_sp - 1):
        head = heads[k]
        size = jnp.exp(rate * float(tok) + head[0:groups, states:2 * states])
        n_re, n_im = times(size * w_re, size * w_im, in_re, in_im)
        n_re = n_re + head[0:groups, 0:states]
        n_im = n_im + head[groups:2 * groups, 0:states]
        in_re = jnp.where(k < me, n_re, in_re)
        in_im = jnp.where(k < me, n_im, in_im)
    for g in range(groups):
        row = slice(g, g + 1)
        c_re, c_im = times(cin_ref[g], cq_ref[g], in_re[row], in_im[row])
        value = (
            loc_r[g]
            + jnp.dot(c_re, cum_r[g], precision=HIGH, preferred_element_type=F32)
            - jnp.dot(c_im, cum_i[g], precision=HIGH, preferred_element_type=F32))
        mx[mt, g * lanes:(g + 1) * lanes, :] = jax.nn.gelu(value).astype(BF16)

    def send_mx(k):
        return remote(mx.at[mt], mx.at[mt], s_mx.at[k], r_mx.at[mt], me, k)

    each(n_tp, mt, lambda k: send_mx(k).start())
    each(n_tp, mt, lambda k: send_dw(k).start())

    def wait_tp(buf, sems):
        each(n_tp, mt, lambda k: remote(
            buf.at[k], buf.at[k], sems.at[k], sems.at[k], me, k).wait_recv())

    local[0].wait()
    local[1].wait()
    local[2].wait()
    wait_tp(wx, r_wx)
    wait_tp(mx, r_mx)
    projected = lax.dot_general(
        mx[...].reshape(n_tp * chan, tok), wx[...].reshape(n_tp * chan, d_local),
        (((0,), (0,)), ((), ())), preferred_element_type=F32).astype(BF16)
    stream = (skip[...].astype(F32) + projected.astype(F32)).astype(BF16)
    stream_f = stream.astype(F32)
    stream_s[...] = stream_f
    squares = to_row(jnp.sum(stream_f * stream_f, axis=1, keepdims=True))
    ss[mt] = jnp.broadcast_to(squares, (8, tok))

    scaled = (stream_f * gain[...]).astype(BF16)
    sent = lax.dot_general(
        disp[...], scaled, (((0,), (0,)), ((), ())),
        preferred_element_type=F32).astype(BF16).reshape(n_sp, cap, d_local)
    xs[...] = sent

    def rows_of(k):
        return pl.ds(pl.multiple_of(k * cap, cap), cap)

    def send_rows(k):
        return remote(
            xs.at[k], g_buf.at[mt, rows_of(me), :], s_dis.at[k], r_dis.at[me], k, mt)

    each(n_sp, me, lambda k: send_rows(k).start())
    own_rows = pltpu.make_async_copy(xs.at[me], g_buf.at[mt, rows_of(me), :], l_sem.at[6])
    own_rows.start()

    def send_ss(k):
        return remote(ss.at[mt], ss.at[mt], s_ss.at[k], r_ss.at[mt], me, k)

    each(n_tp, mt, lambda k: send_ss(k).start())
    wait_tp(ss, r_ss)
    norm = lax.rsqrt(jnp.sum(ss[...], axis=0)[0:1, :] * (1.0 / width) + EPS)
    norm_x = jnp.sum(disp[...].astype(F32) * to_col(norm), axis=0, keepdims=True)
    for k in range(slots // 128):
        inv[k] = jnp.broadcast_to(norm_x[:, k * 128:(k + 1) * 128], (8, 128))

    def tile_of(k):
        return (k * cap) // 128

    def send_inv(k):
        return remote(
            inv.at[tile_of(k)], rinv.at[me], s_inv.at[k], r_inv.at[me], k, mt)

    each(n_sp, me, lambda k: send_inv(k).start())
    rinv[me] = inv[tile_of(me)]

    def inv_of(q):
        part = rinv[q * sp_q:(q + 1) * sp_q]
        full = jnp.concatenate([part] * (cap // 8), axis=1).reshape(rows_q, 128)
        want = (me * cap) % 128 + jnp.bitwise_and(iota((rows_q, 128), 0), cap - 1)
        return jnp.sum(jnp.where(iota((rows_q, 128), 1) == want, full, 0.0), axis=1, keepdims=True)

    def hops(q):
        far, near = n_y // 2, n_y - 1 - n_y // 2
        return (far, near) if q % 2 == 0 else (near, far)

    deepest = n_y // 2

    def chip(k):
        return lax.rem(y + k + n_y, n_y)

    started = []

    def ring_hop(buf, send, recv, q, h):
        rows = pl.ds(q * rows_q, rows_q)

        def push(owner, tp, slot):
            copy = remote(
                buf.at[owner, rows, :], buf.at[owner, rows, :],
                send.at[slot, q], recv.at[owner, q], me, tp)
            copy.start()
            started.append(copy)

        def arrived(owner):
            remote(
                buf.at[owner, rows, :], buf.at[owner, rows, :],
                send.at[0, q], recv.at[owner, q], me, mt).wait_recv()

        right, left = hops(q)
        right_tp, left_tp = chip(1) * CORES + core, chip(-1) * CORES + core
        if h == 0:
            push(mt, right_tp, 0)
            push(mt, left_tp, 1)
            push(mt, twin, 2)
            return
        if h <= right:
            owner = chip(-h) * CORES + core
            arrived(owner)
            if h < right:
                push(owner, right_tp, 3 * h)
            push(owner, twin, 3 * h + 2)
        if h <= left:
            owner = chip(h) * CORES + core
            arrived(owner)
            if h < left:
                push(owner, left_tp, 3 * h + 1)
            push(owner, twin, 3 * (deepest + 1) + h)

    def pairs(buf, send, recv, q, h, weights, target, deep):
        rows = pl.ds(q * rows_q, rows_q)
        right, left = hops(q)
        owners = [0] if h == 0 else [-h] * (h <= right) + [h] * (h <= left)
        for k in owners:
            there = chip(k)
            other = there * CORES + (1 - core)
            remote(
                buf.at[other, rows, :], buf.at[other, rows, :],
                send.at[0, q], recv.at[other, q], me, mt).wait_recv()
            both = jnp.concatenate(
                [buf[there * CORES, rows, :], buf[there * CORES + 1, rows, :]], axis=1)
            part = jnp.dot(both, weights(there), preferred_element_type=F32)
            if h == 0:
                target[rows, :] = part
            else:
                target[rows, :] += part

    def gate_up(there):
        depth = CORES * d_local
        return gu[pl.ds(pl.multiple_of(there * depth, depth), depth), :]

    def down(there):
        return jnp.concatenate([dw[there * CORES], dw[there * CORES + 1]], axis=0)

    def send_back(k):
        return remote(
            outb.at[rows_of(k), :], ret.at[rows_of(me), :], s_ret.at[k], r_ret.at[me], k, mt)

    own_back = pltpu.make_async_copy(
        outb.at[rows_of(me), :], ret.at[rows_of(me), :], l_sem.at[7])

    def stage(q, st):
        rows = slice(q * rows_q, (q + 1) * rows_q)
        first = deepest + 1
        if st == 0:
            def got(k):
                @pl.when(k != me)
                def _():
                    remote(
                        xs.at[0], g_buf.at[mt, rows_of(k), :], s_dis.at[k], r_dis.at[k],
                        me, mt).wait_recv()

                @pl.when(k == me)
                def _():
                    own_rows.wait()
            span(q * sp_q, (q + 1) * sp_q, got)
            ring_hop(g_buf, s_g, r_g, q, 0)
        elif st <= deepest:
            ring_hop(g_buf, s_g, r_g, q, st)
            pairs(g_buf, s_g, r_g, q, st - 1, gate_up, acc, None)
        elif st == first:
            pairs(g_buf, s_g, r_g, q, deepest, gate_up, acc, None)
            factor = inv_of(q)
            gate = acc[rows, 0:f_local] * factor
            wide = acc[rows, f_local:2 * f_local] * factor
            h_buf[mt, rows, :] = (jax.nn.silu(gate) * wide).astype(BF16)
            ring_hop(h_buf, s_h, r_h, q, 0)
        elif st <= first + deepest:
            ring_hop(h_buf, s_h, r_h, q, st - first)
            pairs(h_buf, s_h, r_h, q, st - first - 1, down, oacc, None)
        else:
            pairs(h_buf, s_h, r_h, q, deepest, down, oacc, None)
            outb[rows, :] = oacc[rows, :].astype(BF16)

            def back(k):
                @pl.when(k != me)
                def _():
                    send_back(k).start()

                @pl.when(k == me)
                def _():
                    own_back.start()
            span(q * sp_q, (q + 1) * sp_q, back)

    last_stage = 2 * deepest + 2
    order = sorted((st + SKEW * q, q, st) for q in range(CHUNKS) for st in range(last_stage + 1))
    ready = {0: False, 1: False}
    for _, q, st in order:
        if st == 1 and not ready[0]:
            local[3].wait()
            local[4].wait()
            ready[0] = True
        if st == deepest + 1 and not ready[1]:
            each(n_sp, me, lambda k: remote(
                inv.at[0], rinv.at[k], s_inv.at[k], r_inv.at[k], me, mt).wait_recv())
            local[5].wait()
            wait_tp(dw, r_dw)
            ready[1] = True
        stage(q, st)

    own_back.wait()
    each(n_sp, me, lambda k: remote(
        outb.at[rows_of(k), :], ret.at[rows_of(k), :], s_ret.at[k], r_ret.at[k],
        me, mt).wait_recv())
    back = ret[...]
    out_ref[...] = (
        stream_s[...]
        + jnp.dot(whi[...], back, preferred_element_type=F32)
        + jnp.dot(wlo[...], back, preferred_element_type=F32)).astype(BF16)

    span(me + 1, n_sp, lambda k: send_head(k).wait_send())
    for fn in (send_wx, send_mx, send_dw, send_ss):
        each(n_tp, mt, lambda k: fn(k).wait_send())
    for fn in (send_rows, send_inv, send_back):
        each(n_sp, me, lambda k: fn(k).wait_send())
    for copy in started:
        copy.wait_send()


def per_device(
    lane_source_signal, spectral_damping_part, spectral_angular_part, interval_exponent,
    entry_matrix_inphase, entry_matrix_quadrature, emission_inphase, emission_quadrature,
    lane_bypass_factor, spike_shrink_offset, lane_exit_matrix, skipline_stream,
    specialist_scaling_vector, selected_specialists, dispatcher_scores,
    specialist_valve_matrix, specialist_widen_matrix, specialist_shrink_matrix,
):
    n_sp, n_tp = lax.axis_size("sp"), lax.axis_size("tp")
    groups, states, lanes = entry_matrix_inphase.shape
    chan, tok = lane_source_signal.shape
    width = specialist_scaling_vector.shape[0]
    d_local = width // n_tp
    f_local = specialist_valve_matrix.shape[2]
    cap = 2 * tok * selected_specialists.shape[1] // n_sp
    slots = n_sp * cap
    deepest = n_tp // CORES // 2
    dims = (n_sp, n_tp, groups, states, lanes, tok, width, cap)
    vmem = pl.BlockSpec(memory_space=pltpu.VMEM)
    hbm = pl.BlockSpec(memory_space=pl.ANY)
    dma = pltpu.SemaphoreType.DMA
    scratch = [
        pltpu.VMEM((8, 128), F32),
        pltpu.VMEM((n_sp, 8, 128), F32),
        pltpu.VMEM((n_tp, chan, d_local), BF16),
        pltpu.VMEM((n_tp, chan, tok), BF16),
        pltpu.VMEM((n_tp, f_local, d_local), BF16),
        pltpu.VMEM((width, 2 * f_local), BF16),
        pltpu.VMEM((tok, d_local), BF16),
        pltpu.VMEM((1, d_local), F32),
        pltpu.VMEM((n_tp, 8, tok), F32),
        pltpu.VMEM((slots // 128, 8, 128), F32),
        pltpu.VMEM((n_sp, 8, 128), F32),
        pltpu.VMEM((tok, slots), BF16),
        pltpu.VMEM((tok, slots), BF16),
        pltpu.VMEM((tok, slots), BF16),
        pltpu.VMEM((n_sp, cap, d_local), BF16),
        pltpu.VMEM((n_tp, slots, d_local), BF16),
        pltpu.VMEM((n_tp, slots, f_local), BF16),
        pltpu.VMEM((slots, 2 * f_local), F32),
        pltpu.VMEM((slots, d_local), F32),
        pltpu.VMEM((slots, d_local), BF16),
        pltpu.VMEM((slots, d_local), BF16),
        pltpu.VMEM((tok, d_local), F32),
        pltpu.VMEM((groups, lanes, tok), F32),
        pltpu.VMEM((groups, states, tok), F32),
        pltpu.VMEM((groups, states, tok), F32),
        dma((8,)),
        dma((n_sp,)), dma((n_sp,)),
        dma((n_tp,)), dma((n_tp,)), dma((n_tp,)), dma((n_tp,)),
        dma((n_tp,)), dma((n_tp,)), dma((n_tp,)), dma((n_tp,)),
        dma((n_sp,)), dma((n_sp,)), dma((n_sp,)), dma((n_sp,)), dma((n_sp,)), dma((n_sp,)),
        dma((4 * deepest + 4, CHUNKS)), dma((n_tp, CHUNKS)),
        dma((4 * deepest + 4, CHUNKS)), dma((n_tp, CHUNKS)),
    ]
    return pl.pallas_call(
        functools.partial(mixer_kernel, dims),
        out_shape=jax.ShapeDtypeStruct((tok, d_local), BF16),
        in_specs=[vmem] * 12 + [hbm] * 6,
        out_specs=vmem,
        scratch_shapes=scratch,
        compiler_params=pltpu.CompilerParams(
            collective_id=0, has_side_effects=True, vmem_limit_bytes=60 * 1024 * 1024),
    )(
        lane_source_signal, spectral_damping_part, spectral_angular_part,
        interval_exponent.reshape(1, groups), entry_matrix_inphase, entry_matrix_quadrature,
        emission_inphase, emission_quadrature, lane_bypass_factor.reshape(1, chan),
        spike_shrink_offset, selected_specialists, dispatcher_scores, lane_exit_matrix,
        skipline_stream, specialist_scaling_vector.reshape(1, width),
        specialist_valve_matrix, specialist_widen_matrix, specialist_shrink_matrix,
    )


def solution(mesh):
    placed = (
        P("tp", "sp"), P("tp", None), P("tp", None), P("tp"), P("tp", None, None),
        P("tp", None, None), P("tp", None, None), P("tp", None, None), P("tp"),
        P("tp", "sp"), P("tp", None), P("sp", None), P(), P("sp", None), P("sp", None),
        P("sp", None, "tp"), P("sp", None, "tp"), P("sp", "tp", None),
    )
    return jax.shard_map(
        per_device, mesh=mesh, in_specs=placed, out_specs=P("sp", "tp"), check_vma=False
    )
```

```python
import functools

import jax
import jax.numpy as jnp
from jax import lax
from jax.experimental import pallas as pl
from jax.experimental.pallas import tpu as pltpu
from jax.sharding import PartitionSpec as P

EPS = 1e-06
HIGH = lax.Precision.HIGHEST
MESH = pl.DeviceIdType.MESH
F32 = jnp.float32
BF16 = jnp.bfloat16
CORES = 2
CHUNKS = 4
SKEW = 0.5
X_CHIPS = 4
DW_EARLY = 2


def iota(shape, dim):
    return lax.broadcasted_iota(jnp.int32, shape, dim)


def to_col(row):
    n = row.shape[1]
    eye = iota((n, n), 0) == iota((n, n), 1)
    return jnp.sum(jnp.where(eye, row, 0.0), axis=1, keepdims=True)


def to_row(col):
    n = col.shape[0]
    eye = iota((n, n), 0) == iota((n, n), 1)
    return jnp.sum(jnp.where(eye, col, 0.0), axis=0, keepdims=True)


def small_expm1(x):
    total = jnp.ones_like(x)
    for k in range(11, 1, -1):
        total = 1.0 + total * x * (1.0 / k)
    return jnp.where(x > -0.7, x * total, jnp.exp(x) - 1.0)


def dot_first(a, b):
    return lax.dot_general(
        a, b, (((0,), (0,)), ((), ())), precision=HIGH, preferred_element_type=F32)


def times(ar, ai, br, bi):
    return ar * br - ai * bi, ar * bi + ai * br


def mixer_kernel(
    dims,
    u_ref, damp_ref, ang_ref, ie_ref, ein_ref, eq_ref, cin_ref, cq_ref, byp_ref, off_ref,
    sel_ref, score_ref, wexit_hbm, skip_hbm, gain_hbm, gate_hbm, up_hbm, down_hbm,
    out_ref,
    msg, heads, wx, mx, dw, gu, skip, gain, ss, inv, rinv, disp, whi, wlo,
    xs, g_buf, h_buf, acc, oacc, outb, ret, stream_s, loc_r, cum_r, cum_i,
    l_sem, s_pre, r_pre, s_wx, r_wx, s_wq, r_wq, s_mx, r_mx, s_dw, r_dw, s_ss, r_ss,
    s_inv, r_inv, s_dis, r_dis, s_ret, r_ret, s_g, r_g, s_h, r_h,
):
    n_sp, n_tp, groups, states, lanes, tok, width, cap = dims
    n_y = n_tp // CORES
    d_local = width // n_tp
    f_local = gate_hbm.shape[2]
    slots = n_sp * cap
    rows_q = slots // CHUNKS
    sp_q = n_sp // CHUNKS
    me, mt = lax.axis_index("sp"), lax.axis_index("tp")
    y, core = mt // CORES, mt % CORES
    twin = y * CORES + (1 - core)
    x_part = me % X_CHIPS
    away = [k for d in range(1, n_y // 2 + 1) for k in ((d, -d) if 2 * d < n_y else (d,))]

    def chip(k):
        return lax.rem(y + k + n_y, n_y)

    def each(count, mine, fn):
        def step(j, carry):
            fn(lax.rem(mine + j, count))
            return carry
        lax.fori_loop(1, count, step, 0)

    def span(lo, hi, fn):
        def step(j, carry):
            fn(j)
            return carry
        lax.fori_loop(lo, hi, step, 0)

    def remote(src, dst, send, recv, sp, tp):
        return pltpu.make_async_remote_copy(
            src_ref=src, dst_ref=dst, send_sem=send, recv_sem=recv,
            device_id=(sp, tp), device_id_type=MESH)

    scope = []

    def mark(name):
        if scope:
            scope.pop().__exit__(None, None, None)
        if name:
            scope.append(jax.named_scope(name))
            scope[-1].__enter__()

    heads[...] = jnp.zeros_like(heads)
    barrier = pltpu.get_barrier_semaphore()
    each(n_sp, me, lambda k: pl.semaphore_signal(
        barrier, inc=1, device_id=(k, mt), device_id_type=MESH))
    each(n_tp, mt, lambda k: pl.semaphore_signal(
        barrier, inc=1, device_id=(me, k), device_id_type=MESH))

    mark("local_copies")
    own_cols = pl.ds(pl.multiple_of(mt * d_local, d_local), d_local)
    chan = groups * lanes
    part = chan // X_CHIPS
    quarter = pl.ds(pl.multiple_of(x_part * part, part), part)
    local = [
        pltpu.make_async_copy(skip_hbm.at[:, own_cols], skip, l_sem.at[0]),
        pltpu.make_async_copy(gain_hbm.at[:, own_cols], gain, l_sem.at[1]),
        pltpu.make_async_copy(
            wexit_hbm.at[quarter, own_cols], wx.at[mt, quarter, :], l_sem.at[2]),
        pltpu.make_async_copy(gate_hbm.at[0], gu.at[:, pl.ds(0, f_local)], l_sem.at[3]),
        pltpu.make_async_copy(up_hbm.at[0], gu.at[:, pl.ds(f_local, f_local)], l_sem.at[4]),
        pltpu.make_async_copy(down_hbm.at[0, :, own_cols], dw.at[mt], l_sem.at[5]),
    ]
    for copy in local:
        copy.start()

    mark("state")
    step_size = jnp.exp(to_col(ie_ref[...]))
    damp, ang = damp_ref[...], ang_ref[...]
    rate, angle = damp * step_size, ang * step_size
    cos, sin = jnp.cos(angle), jnp.sin(angle)
    half = jnp.sin(0.5 * angle)
    num_re = small_expm1(rate) * cos - 2.0 * half * half
    num_im = jnp.exp(rate) * sin
    denom = damp * damp + ang * ang
    fac_re = (num_re * damp + num_im * ang) / denom
    fac_im = (num_im * damp - num_re * ang) / denom
    total = off_ref[...]
    lane_g = iota(total.shape, 1)
    shift = 1
    while shift < tok:
        total = total + jnp.where(lane_g >= shift, pltpu.roll(total, shift, 1), 0.0)
        shift *= 2
    lane = iota((states, tok), 1)
    bypass = byp_ref[...]
    for g in range(groups):
        row = slice(g, g + 1)
        u = u_ref[g * lanes:(g + 1) * lanes, :].astype(F32)
        e_re = dot_first(ein_ref[g], u)
        e_im = dot_first(eq_ref[g], u)
        f_re, f_im = to_col(fac_re[row]), to_col(fac_im[row])
        s_re, s_im = times(f_re, f_im, e_re, e_im)
        rate_c = to_col(rate[row])
        w_re, w_im = to_col(cos[row]), to_col(sin[row])
        sums = total[row]
        p_re, p_im = jnp.ones((states, tok), F32), jnp.zeros((states, tok), F32)
        shift = 1
        while shift <= tok:
            taken = (jnp.bitwise_and(lane + 1, shift)) != 0
            q_re, q_im = times(p_re, p_im, w_re, w_im)
            p_re, p_im = jnp.where(taken, q_re, p_re), jnp.where(taken, q_im, p_im)
            if shift < tok:
                gap = sums - pltpu.roll(sums, shift, 1)
                size = jnp.exp(rate_c * float(shift) + jnp.minimum(gap, 0.0))
                size = jnp.where(lane >= shift, size, 0.0)
                t_re, t_im = times(
                    w_re, w_im, pltpu.roll(s_re, shift, 1), pltpu.roll(s_im, shift, 1))
                s_re, s_im = s_re + size * t_re, s_im + size * t_im
                w_re, w_im = times(w_re, w_im, w_re, w_im)
            shift *= 2
        size = jnp.exp(rate_c * (lane + 1).astype(F32) + sums)
        cum_r[g], cum_i[g] = size * p_re, size * p_im
        last = lane == tok - 1
        h_re = to_row(jnp.sum(jnp.where(last, s_re, 0.0), axis=1, keepdims=True))
        h_im = to_row(jnp.sum(jnp.where(last, s_im, 0.0), axis=1, keepdims=True))
        end = jnp.sum(jnp.where(lane_g[row] == tok - 1, sums, 0.0), axis=1, keepdims=True)
        msg[g:g + 1, 0:states] = h_re
        msg[g:g + 1, states:2 * states] = jnp.broadcast_to(end, (1, states))
        msg[groups + g:groups + g + 1, 0:states] = h_im
        msg[groups + g:groups + g + 1, states:2 * states] = jnp.zeros((1, states), F32)
        loc_r[g] = (
            jnp.dot(cin_ref[g], s_re, precision=HIGH, preferred_element_type=F32)
            - jnp.dot(cq_ref[g], s_im, precision=HIGH, preferred_element_type=F32)
            + to_col(bypass[:, g * lanes:(g + 1) * lanes]) * u)

    mark("barrier")
    pl.semaphore_wait(barrier, n_sp - 1 + n_tp - 1)

    def send_head(k):
        return remote(msg, heads.at[me], s_pre.at[k], r_pre.at[me], k, mt)

    def head_from(k):
        return remote(msg, heads.at[k], s_pre.at[k], r_pre.at[k], me, mt)

    mark("send_head")
    span(me + 1, n_sp, lambda k: send_head(k).start())

    def columns_of(k):
        return pl.ds(pl.multiple_of(k * d_local, d_local), d_local)

    def send_wx(k):
        return remote(
            wexit_hbm.at[quarter, columns_of(k)], wx.at[mt, quarter, :],
            s_wx, r_wx.at[mt], me, k)

    def quarter_of(j):
        other = (x_part + j) % X_CHIPS
        rows = pl.ds(pl.multiple_of(other * part, part), part)
        return me - x_part + other, wx.at[:, rows, :], other

    def send_quarter(j):
        there, _, _ = quarter_of(j)
        mine = wx.at[:, quarter, :]
        return remote(mine, mine, s_wq, r_wq.at[x_part], there, mt)

    def send_dw(k):
        return remote(
            down_hbm.at[0, :, columns_of(k)], dw.at[mt], s_dw, r_dw.at[mt], me, k)

    def send_dw_to(d):
        for c in range(CORES):
            send_dw(chip(d) * CORES + c).start()

    mark("send_wx")
    each(n_tp, mt, lambda k: send_wx(k).start())
    for d in away[:DW_EARLY]:
        send_dw_to(d)

    mark("routing")
    sel, score = sel_ref[...].astype(F32), score_ref[...]
    expert = iota((tok, n_sp), 1).astype(F32)
    hit0 = (to_col(sel[0:1]) == expert).astype(F32)
    hit1 = (to_col(sel[1:2]) == expert).astype(F32)
    hits = (hit0 + hit1).astype(BF16)
    below = (iota((tok, tok), 1) < iota((tok, tok), 0)).astype(F32).astype(BF16)
    rank = jnp.dot(below, hits, preferred_element_type=F32).astype(BF16)
    slot_e, slot_j = iota((n_sp, slots), 0), iota((n_sp, slots), 1)
    spread = ((slot_j >= slot_e * cap) & (slot_j < (slot_e + 1) * cap)).astype(F32).astype(BF16)
    hits_x = jnp.dot(hits, spread, preferred_element_type=F32)
    hit0_x = jnp.dot(hit0.astype(BF16), spread, preferred_element_type=F32)
    rank_x = jnp.dot(rank, spread, preferred_element_type=F32)
    place = jnp.bitwise_and(iota((tok, slots), 1), cap - 1).astype(F32)
    picked = (hits_x > 0.5) & (rank_x == place)
    disp[...] = picked.astype(F32).astype(BF16)
    both = score[0:1] + score[1:2]
    share = jnp.where(hit0_x > 0.5, to_col(score[0:1] / both), to_col(score[1:2] / both))
    share = jnp.where(picked, share, 0.0)
    high = share.astype(BF16)
    whi[...] = high
    wlo[...] = (share - high.astype(F32)).astype(BF16)

    mark("wait_head")
    span(0, me, lambda k: head_from(k).wait_recv())
    mark("enter")
    w_re, w_im = cos, sin
    shift = 1
    while shift < tok:
        w_re, w_im = times(w_re, w_im, w_re, w_im)
        shift *= 2
    in_re, in_im = jnp.zeros_like(rate), jnp.zeros_like(rate)
    for k in range(n_sp - 1):
        head = heads[k]
        size = jnp.exp(rate * float(tok) + head[0:groups, states:2 * states])
        n_re, n_im = times(size * w_re, size * w_im, in_re, in_im)
        n_re = n_re + head[0:groups, 0:states]
        n_im = n_im + head[groups:2 * groups, 0:states]
        in_re = jnp.where(k < me, n_re, in_re)
        in_im = jnp.where(k < me, n_im, in_im)
    for g in range(groups):
        row = slice(g, g + 1)
        c_re, c_im = times(cin_ref[g], cq_ref[g], in_re[row], in_im[row])
        value = (
            loc_r[g]
            + jnp.dot(c_re, cum_r[g], precision=HIGH, preferred_element_type=F32)
            - jnp.dot(c_im, cum_i[g], precision=HIGH, preferred_element_type=F32))
        mx[mt, g * lanes:(g + 1) * lanes, :] = jax.nn.gelu(value).astype(BF16)

    def send_mx(owner, tp):
        return remote(mx.at[owner], mx.at[owner], s_mx, r_mx.at[owner], me, tp)

    mark("send_mx")
    for d in away:
        send_mx(mt, chip(d) * CORES + core).start()
    send_mx(mt, twin).start()

    def got(dst, sem):
        remote(dst, dst, s_mx, sem, me, twin).wait_recv()

    mark("wait_quarter")
    local[2].wait()
    each(n_tp, mt, lambda k: got(wx.at[k, quarter, :], r_wx.at[k]))
    for j in range(1, X_CHIPS):
        send_quarter(j).start()
    for d in away[DW_EARLY:]:
        send_dw_to(d)
    send_dw(twin).start()

    mark("relay_mx")
    local[0].wait()
    local[1].wait()
    for d in away:
        owner = chip(-d) * CORES + core
        got(mx.at[owner], r_mx.at[owner])
        send_mx(owner, twin).start()
    mark("wait_wq")
    for j in range(1, X_CHIPS):
        _, dst, other = quarter_of(j)
        got(dst, r_wq.at[other])
    mark("wait_mx")
    for d in [0] + away:
        owner = chip(-d) * CORES + (1 - core)
        got(mx.at[owner], r_mx.at[owner])
    mark("project")
    projected = lax.dot_general(
        mx[...].reshape(n_tp * chan, tok), wx[...].reshape(n_tp * chan, d_local),
        (((0,), (0,)), ((), ())), preferred_element_type=F32).astype(BF16)
    stream = (skip[...].astype(F32) + projected.astype(F32)).astype(BF16)
    stream_f = stream.astype(F32)
    stream_s[...] = stream_f
    squares = to_row(jnp.sum(stream_f * stream_f, axis=1, keepdims=True))
    ss[mt] = jnp.broadcast_to(squares, (8, tok))

    scaled = (stream_f * gain[...]).astype(BF16)
    sent = lax.dot_general(
        disp[...], scaled, (((0,), (0,)), ((), ())),
        preferred_element_type=F32).astype(BF16).reshape(n_sp, cap, d_local)
    xs[...] = sent

    def rows_of(k):
        return pl.ds(pl.multiple_of(k * cap, cap), cap)

    def send_rows(k):
        return remote(
            xs.at[k], g_buf.at[mt, rows_of(me), :], s_dis, r_dis.at[me], k, mt)

    mark("send_rows")
    each(n_sp, me, lambda k: send_rows(k).start())
    own_rows = pltpu.make_async_copy(xs.at[me], g_buf.at[mt, rows_of(me), :], l_sem.at[6])
    own_rows.start()

    one = pl.ds(0, 1)

    def send_ss(k):
        mine = ss.at[mt, one, :]
        return remote(mine, mine, s_ss, r_ss.at[mt], me, k)

    each(n_tp, mt, lambda k: send_ss(k).start())

    def tile_of(k):
        return (k * cap) // 128

    def send_inv(k):
        return remote(
            inv.at[tile_of(k), one, :], rinv.at[me, one, :], s_inv, r_inv.at[me], k, mt)

    def norm_factors():
        mark("wait_ss")
        each(n_tp, mt, lambda k: got(ss.at[k, one, :], r_ss.at[k]))
        mark("norm")
        norm = lax.rsqrt(jnp.sum(ss[...], axis=0)[0:1, :] * (1.0 / width) + EPS)
        norm_x = jnp.sum(disp[...].astype(F32) * to_col(norm), axis=0, keepdims=True)
        for k in range(slots // 128):
            inv[k] = jnp.broadcast_to(norm_x[:, k * 128:(k + 1) * 128], (8, 128))
        each(n_sp, me, lambda k: send_inv(k).start())
        rinv[me] = inv[tile_of(me)]

    def inv_of(q):
        part = rinv[q * sp_q:(q + 1) * sp_q][:, 0:1, :]
        full = jnp.broadcast_to(part, (sp_q, cap, 128)).reshape(rows_q, 128)
        want = (me * cap) % 128 + jnp.bitwise_and(iota((rows_q, 128), 0), cap - 1)
        return jnp.sum(jnp.where(iota((rows_q, 128), 1) == want, full, 0.0), axis=1, keepdims=True)

    def hops(q):
        far, near = n_y // 2, n_y - 1 - n_y // 2
        return (far, near) if q % 2 == 0 else (near, far)

    deepest = n_y // 2

    def ring_hop(buf, send, recv, q, h):
        rows = pl.ds(q * rows_q, rows_q)

        def push(owner, tp):
            there = buf.at[owner, rows, :]
            remote(there, there, send.at[q], recv.at[owner, q], me, tp).start()

        def arrived(owner):
            got(buf.at[owner, rows, :], recv.at[owner, q])

        right, left = hops(q)
        right_tp, left_tp = chip(1) * CORES + core, chip(-1) * CORES + core
        if h == 0:
            push(mt, right_tp)
            push(mt, left_tp)
            push(mt, twin)
            return
        if h <= right:
            owner = chip(-h) * CORES + core
            arrived(owner)
            if h < right:
                push(owner, right_tp)
            push(owner, twin)
        if h <= left:
            owner = chip(h) * CORES + core
            arrived(owner)
            if h < left:
                push(owner, left_tp)
            push(owner, twin)

    def pairs(buf, recv, q, h, weights, target):
        rows = pl.ds(q * rows_q, rows_q)
        right, left = hops(q)
        owners = [0] if h == 0 else [-h] * (h <= right) + [h] * (h <= left)
        for k in owners:
            there = chip(k)
            other = there * CORES + (1 - core)
            got(buf.at[other, rows, :], recv.at[other, q])
            both = jnp.concatenate(
                [buf[there * CORES, rows, :], buf[there * CORES + 1, rows, :]], axis=1)
            part = jnp.dot(both, weights(there), preferred_element_type=F32)
            if h == 0:
                target[rows, :] = part
            else:
                target[rows, :] += part

    def gate_up(there):
        depth = CORES * d_local
        return gu[pl.ds(pl.multiple_of(there * depth, depth), depth), :]

    def down(there):
        return jnp.concatenate([dw[there * CORES], dw[there * CORES + 1]], axis=0)

    def send_back(k):
        return remote(
            outb.at[rows_of(k), :], ret.at[rows_of(me), :], s_ret, r_ret.at[me], k, mt)

    own_back = pltpu.make_async_copy(
        outb.at[rows_of(me), :], ret.at[rows_of(me), :], l_sem.at[7])

    def stage(q, st):
        rows = slice(q * rows_q, (q + 1) * rows_q)
        first = deepest + 1
        if st == 0:
            def arrival(k):
                @pl.when(k != me)
                def _():
                    got(g_buf.at[mt, rows_of(k), :], r_dis.at[k])

                @pl.when(k == me)
                def _():
                    own_rows.wait()
            span(q * sp_q, (q + 1) * sp_q, arrival)
            ring_hop(g_buf, s_g, r_g, q, 0)
        elif st <= deepest:
            ring_hop(g_buf, s_g, r_g, q, st)
            pairs(g_buf, r_g, q, st - 1, gate_up, acc)
        elif st == first:
            pairs(g_buf, r_g, q, deepest, gate_up, acc)
            factor = inv_of(q)
            gate = acc[rows, 0:f_local] * factor
            wide = acc[rows, f_local:2 * f_local] * factor
            h_buf[mt, rows, :] = (jax.nn.silu(gate) * wide).astype(BF16)
            ring_hop(h_buf, s_h, r_h, q, 0)
        elif st <= first + deepest:
            ring_hop(h_buf, s_h, r_h, q, st - first)
            pairs(h_buf, r_h, q, st - first - 1, down, oacc)
        else:
            pairs(h_buf, r_h, q, deepest, down, oacc)
            outb[rows, :] = oacc[rows, :].astype(BF16)

            def back(k):
                @pl.when(k != me)
                def _():
                    send_back(k).start()

                @pl.when(k == me)
                def _():
                    own_back.start()
            span(q * sp_q, (q + 1) * sp_q, back)

    last_stage = 2 * deepest + 2
    order = sorted(
        (st + SKEW * q if st else -1, q, st) for q in range(CHUNKS) for st in range(last_stage + 1))
    ready = [False] * 3
    for _, q, st in order:
        if st == 1 and not ready[0]:
            local[3].wait()
            local[4].wait()
            ready[0] = True
        if st == 3 and not ready[2]:
            norm_factors()
            ready[2] = True
        if st == deepest + 1 and not ready[1]:
            mark("wait_inv")
            each(n_sp, me, lambda k: got(rinv.at[k, one, :], r_inv.at[k]))
            mark("wait_dw")
            local[5].wait()
            each(n_tp, mt, lambda k: got(dw.at[k], r_dw.at[k]))
            ready[1] = True
        mark(f"stage#t={st + SKEW * q}#q={q}#st={st}")
        stage(q, st)

    mark("wait_back")
    own_back.wait()
    each(n_sp, me, lambda k: got(ret.at[rows_of(k), :], r_ret.at[k]))
    mark("combine")
    back = ret[...]
    out_ref[...] = (
        stream_s[...]
        + jnp.dot(whi[...], back, preferred_element_type=F32)
        + jnp.dot(wlo[...], back, preferred_element_type=F32)).astype(BF16)

    mark("drain")
    span(me + 1, n_sp, lambda k: send_head(k).wait_send())

    def sent_all(view, sem):
        remote(view, view, sem, sem, me, twin).wait_send()

    sent_all(wx.at[pl.ds(0, n_tp - 1), quarter, :], s_wx)
    sent_all(wx.at[:, pl.ds(0, part * (X_CHIPS - 1)), :], s_wq)
    sent_all(mx.at[pl.ds(0, 2 * n_y - 1)], s_mx)
    sent_all(dw.at[pl.ds(0, n_tp - 1)], s_dw)
    sent_all(ss.at[pl.ds(0, n_tp - 1), one, :], s_ss)
    sent_all(xs.at[pl.ds(0, n_sp - 1)], s_dis)
    sent_all(rinv.at[pl.ds(0, n_sp - 1), one, :], s_inv)
    sent_all(outb.at[pl.ds(0, (n_sp - 1) * cap), :], s_ret)
    for q in range(CHUNKS):
        rows = pl.ds(q * rows_q, rows_q)
        sent_all(g_buf.at[pl.ds(0, 2 * n_y - 1), rows, :], s_g.at[q])
        sent_all(h_buf.at[pl.ds(0, 2 * n_y - 1), rows, :], s_h.at[q])
    mark(None)


def per_device(
    lane_source_signal, spectral_damping_part, spectral_angular_part, interval_exponent,
    entry_matrix_inphase, entry_matrix_quadrature, emission_inphase, emission_quadrature,
    lane_bypass_factor, spike_shrink_offset, lane_exit_matrix, skipline_stream,
    specialist_scaling_vector, selected_specialists, dispatcher_scores,
    specialist_valve_matrix, specialist_widen_matrix, specialist_shrink_matrix,
):
    n_sp, n_tp = lax.axis_size("sp"), lax.axis_size("tp")
    groups, states, lanes = entry_matrix_inphase.shape
    chan, tok = lane_source_signal.shape
    width = specialist_scaling_vector.shape[0]
    d_local = width // n_tp
    f_local = specialist_valve_matrix.shape[2]
    cap = 2 * tok * selected_specialists.shape[1] // n_sp
    slots = n_sp * cap
    dims = (n_sp, n_tp, groups, states, lanes, tok, width, cap)
    vmem = pl.BlockSpec(memory_space=pltpu.VMEM)
    hbm = pl.BlockSpec(memory_space=pl.ANY)
    dma = pltpu.SemaphoreType.DMA
    scratch = [
        pltpu.VMEM((8, 128), F32),
        pltpu.VMEM((n_sp, 8, 128), F32),
        pltpu.VMEM((n_tp, chan, d_local), BF16),
        pltpu.VMEM((n_tp, chan, tok), BF16),
        pltpu.VMEM((n_tp, f_local, d_local), BF16),
        pltpu.VMEM((width, 2 * f_local), BF16),
        pltpu.VMEM((tok, d_local), BF16),
        pltpu.VMEM((1, d_local), F32),
        pltpu.VMEM((n_tp, 8, tok), F32),
        pltpu.VMEM((slots // 128, 8, 128), F32),
        pltpu.VMEM((n_sp, 8, 128), F32),
        pltpu.VMEM((tok, slots), BF16),
        pltpu.VMEM((tok, slots), BF16),
        pltpu.VMEM((tok, slots), BF16),
        pltpu.VMEM((n_sp, cap, d_local), BF16),
        pltpu.VMEM((n_tp, slots, d_local), BF16),
        pltpu.VMEM((n_tp, slots, f_local), BF16),
        pltpu.VMEM((slots, 2 * f_local), F32),
        pltpu.VMEM((slots, d_local), F32),
        pltpu.VMEM((slots, d_local), BF16),
        pltpu.VMEM((slots, d_local), BF16),
        pltpu.VMEM((tok, d_local), F32),
        pltpu.VMEM((groups, lanes, tok), F32),
        pltpu.VMEM((groups, states, tok), F32),
        pltpu.VMEM((groups, states, tok), F32),
        dma((8,)),
        dma((n_sp,)), dma((n_sp,)),
        dma, dma((n_tp,)), dma, dma((X_CHIPS,)), dma, dma((n_tp,)), dma, dma((n_tp,)),
        dma, dma((n_tp,)), dma, dma((n_sp,)), dma, dma((n_sp,)), dma, dma((n_sp,)),
        dma((CHUNKS,)), dma((n_tp, CHUNKS)), dma((CHUNKS,)), dma((n_tp, CHUNKS)),
    ]
    return pl.pallas_call(
        functools.partial(mixer_kernel, dims),
        out_shape=jax.ShapeDtypeStruct((tok, d_local), BF16),
        in_specs=[vmem] * 12 + [hbm] * 6,
        out_specs=vmem,
        scratch_shapes=scratch,
        compiler_params=pltpu.CompilerParams(
            collective_id=0, has_side_effects=True, vmem_limit_bytes=60 * 1024 * 1024),
    )(
        lane_source_signal, spectral_damping_part, spectral_angular_part,
        interval_exponent.reshape(1, groups), entry_matrix_inphase.transpose(0, 2, 1),
        entry_matrix_quadrature.transpose(0, 2, 1),
        emission_inphase, emission_quadrature, lane_bypass_factor.reshape(1, chan),
        spike_shrink_offset, selected_specialists.T, dispatcher_scores.T, lane_exit_matrix,
        skipline_stream, specialist_scaling_vector.reshape(1, width),
        specialist_valve_matrix, specialist_widen_matrix, specialist_shrink_matrix,
    )


def solution(mesh):
    placed = (
        P("tp", "sp"), P("tp", None), P("tp", None), P("tp"), P("tp", None, None),
        P("tp", None, None), P("tp", None, None), P("tp", None, None), P("tp"),
        P("tp", "sp"), P("tp", None), P("sp", None), P(), P("sp", None), P("sp", None),
        P("sp", None, "tp"), P("sp", None, "tp"), P("sp", "tp", None),
    )
    return jax.shard_map(
        per_device, mesh=mesh, in_specs=placed, out_specs=P("sp", "tp"), check_vma=False
    )
```

```python
import functools

import jax
import jax.numpy as jnp
from jax import lax
from jax.experimental import pallas as pl
from jax.experimental.pallas import tpu as pltpu
from jax.sharding import PartitionSpec as P

EPS = 1e-06
HIGH = lax.Precision.HIGHEST
MESH = pl.DeviceIdType.MESH
F32 = jnp.float32
BF16 = jnp.bfloat16
CORES = 2
CHUNKS = 4
SKEW = 0.5
X_CHIPS = 4
DW_EARLY, DW_MID = 4, 12
PIECE = 32
DW_SLOTS = ((2, 3), (3, 3), (0, 4), (1, 4), (2, 4), (3, 4), (0, 6), (1, 6))
CHUNK_ORDER = (0, 1, 2, 3)


def iota(shape, dim):
    return lax.broadcasted_iota(jnp.int32, shape, dim)


def to_col(row):
    n = row.shape[1]
    eye = iota((n, n), 0) == iota((n, n), 1)
    return jnp.sum(jnp.where(eye, row, 0.0), axis=1, keepdims=True)


def to_row(col):
    n = col.shape[0]
    eye = iota((n, n), 0) == iota((n, n), 1)
    return jnp.sum(jnp.where(eye, col, 0.0), axis=0, keepdims=True)


def small_expm1(x):
    total = jnp.ones_like(x)
    for k in range(11, 1, -1):
        total = 1.0 + total * x * (1.0 / k)
    return jnp.where(x > -0.7, x * total, jnp.exp(x) - 1.0)


def dot_first(a, b):
    return lax.dot_general(
        a, b, (((0,), (0,)), ((), ())), precision=HIGH, preferred_element_type=F32)


def times(ar, ai, br, bi):
    return ar * br - ai * bi, ar * bi + ai * br


def mixer_kernel(
    dims,
    u_hbm, damp_hbm, ang_hbm, ie_hbm, ein_hbm, eq_hbm, cin_hbm, cq_hbm, byp_hbm, off_hbm,
    sel_hbm, score_hbm, wexit_hbm, skip_hbm, gain_hbm, gate_hbm, up_hbm, down_hbm,
    out_ref,
    u_ref, damp_ref, ang_ref, ie_ref, ein_ref, eq_ref, cin_ref, cq_ref, byp_ref, off_ref,
    sel_ref, score_ref,
    msg, heads, wx, mx, dw, gu, skip, gain, squares, disp, whi, wlo,
    xs, g_buf, h_buf, acc, oacc, outb, ret, stream_s, loc_r, cum_r, cum_i,
    i_sem, l_sem, s_pre, r_pre, s_wx, r_wx, s_wq, r_wq, s_mx, r_mx, s_dw, r_dw,
    s_dis, r_dis, s_ret, r_ret, *ring_sems,
):
    n_sp, n_tp, groups, states, lanes, tok, width, cap = dims
    n_y = n_tp // CORES
    d_local = width // n_tp
    f_local = gate_hbm.shape[2]
    slots = n_sp * cap
    rows_q = slots // CHUNKS
    sp_q = n_sp // CHUNKS
    me, mt = lax.axis_index("sp"), lax.axis_index("tp")
    y, core = mt // CORES, mt % CORES
    twin = y * CORES + (1 - core)
    x_part = me % X_CHIPS
    away = [k for d in range(1, n_y // 2 + 1) for k in ((d, -d) if 2 * d < n_y else (d,))]

    def chip(k):
        return around(y + k, n_y)

    def around(value, count):
        if count & (count - 1):
            return lax.rem(value + count, count)
        return jnp.bitwise_and(value, count - 1)

    def each(count, mine, fn):
        for j in range(1, count):
            fn(around(mine + j, count))

    n_z = n_sp // X_CHIPS
    near = sorted(
        ((dz, dx) for dz in range(-((n_z - 1) // 2), n_z // 2 + 1)
         for dx in range(-((X_CHIPS - 1) // 2), X_CHIPS // 2 + 1)),
        key=lambda o: (-(abs(o[0]) + abs(o[1])), -abs(o[0]), o))

    def at_offset(dz, dx):
        return around(me // X_CHIPS + dz, n_z) * X_CHIPS + around(x_part + dx, X_CHIPS)

    def place_at(dz, dx):
        back = [
            k for k, (a, b) in enumerate(near)
            if (a + dz) % n_z == 0 and (b + dx) % X_CHIPS == 0]
        return back[0]

    def far_first(fn):
        for dz, dx in near[:-1]:
            fn(dz, dx)

    def span(lo, hi, fn):
        def step(j, carry):
            fn(j)
            return carry
        lax.fori_loop(lo, hi, step, 0)

    def remote(src, dst, send, recv, sp, tp):
        return pltpu.make_async_remote_copy(
            src_ref=src, dst_ref=dst, send_sem=send, recv_sem=recv,
            device_id=(sp, tp), device_id_type=MESH)

    scope = []

    def mark(name):
        if scope:
            scope.pop().__exit__(None, None, None)
        if name:
            scope.append(jax.named_scope(name))
            scope[-1].__enter__()

    small = [
        pltpu.make_async_copy(src, dst, i_sem.at[k])
        for k, (src, dst) in enumerate((
            (ie_hbm, ie_ref), (damp_hbm, damp_ref), (ang_hbm, ang_ref), (off_hbm, off_ref),
            (u_hbm, u_ref), (ein_hbm, ein_ref), (eq_hbm, eq_ref), (cin_hbm, cin_ref),
            (cq_hbm, cq_ref), (byp_hbm, byp_ref), (sel_hbm, sel_ref), (score_hbm, score_ref)))
    ]
    for copy in small:
        copy.start()

    heads[...] = jnp.zeros_like(heads)
    barrier = pltpu.get_barrier_semaphore()
    far_first(lambda dz, dx: pl.semaphore_signal(
        barrier, inc=1, device_id=(at_offset(dz, dx), mt), device_id_type=MESH))
    for d in away[::-1]:
        for c in range(CORES):
            pl.semaphore_signal(
                barrier, inc=1, device_id=(me, chip(d) * CORES + c), device_id_type=MESH)
    pl.semaphore_signal(barrier, inc=1, device_id=(me, twin), device_id_type=MESH)

    mark("local_copies")
    own_cols = pl.ds(pl.multiple_of(mt * d_local, d_local), d_local)
    chan = groups * lanes
    part = chan // X_CHIPS
    quarter = pl.ds(pl.multiple_of(x_part * part, part), part)
    local = [
        pltpu.make_async_copy(skip_hbm.at[:, own_cols], skip, l_sem.at[0]),
        pltpu.make_async_copy(gain_hbm, gain, l_sem.at[1]),
        pltpu.make_async_copy(
            wexit_hbm.at[quarter, own_cols], wx.at[mt, quarter, :], l_sem.at[2]),
        pltpu.make_async_copy(gate_hbm.at[0], gu.at[:, pl.ds(0, f_local)], l_sem.at[3]),
        pltpu.make_async_copy(up_hbm.at[0], gu.at[:, pl.ds(f_local, f_local)], l_sem.at[4]),
        pltpu.make_async_copy(down_hbm.at[0, :, own_cols], dw.at[mt], l_sem.at[5]),
    ]
    for copy in local:
        copy.start()

    mark("state")
    for copy in small:
        copy.wait()
    step_size = jnp.exp(to_col(ie_ref[...]))
    damp, ang = damp_ref[...], ang_ref[...]
    rate, angle = damp * step_size, ang * step_size
    cos, sin = jnp.cos(angle), jnp.sin(angle)
    half = jnp.sin(0.5 * angle)
    num_re = small_expm1(rate) * cos - 2.0 * half * half
    num_im = jnp.exp(rate) * sin
    denom = damp * damp + ang * ang
    fac_re = (num_re * damp + num_im * ang) / denom
    fac_im = (num_im * damp - num_re * ang) / denom
    total = off_ref[...]
    lane_g = iota(total.shape, 1)
    shift = 1
    while shift < tok:
        total = total + jnp.where(lane_g >= shift, pltpu.roll(total, shift, 1), 0.0)
        shift *= 2
    lane = iota((states, tok), 1)
    bypass = byp_ref[...]
    for g in range(groups):
        row = slice(g, g + 1)
        u = u_ref[g * lanes:(g + 1) * lanes, :].astype(F32)
        e_re = dot_first(ein_ref[g], u)
        e_im = dot_first(eq_ref[g], u)
        f_re, f_im = to_col(fac_re[row]), to_col(fac_im[row])
        s_re, s_im = times(f_re, f_im, e_re, e_im)
        rate_c = to_col(rate[row])
        w_re, w_im = to_col(cos[row]), to_col(sin[row])
        sums = total[row]
        p_re, p_im = jnp.ones((states, tok), F32), jnp.zeros((states, tok), F32)
        shift = 1
        while shift <= tok:
            taken = (jnp.bitwise_and(lane + 1, shift)) != 0
            q_re, q_im = times(p_re, p_im, w_re, w_im)
            p_re, p_im = jnp.where(taken, q_re, p_re), jnp.where(taken, q_im, p_im)
            if shift < tok:
                gap = sums - pltpu.roll(sums, shift, 1)
                size = jnp.exp(rate_c * float(shift) + jnp.minimum(gap, 0.0))
                size = jnp.where(lane >= shift, size, 0.0)
                t_re, t_im = times(
                    w_re, w_im, pltpu.roll(s_re, shift, 1), pltpu.roll(s_im, shift, 1))
                s_re, s_im = s_re + size * t_re, s_im + size * t_im
                w_re, w_im = times(w_re, w_im, w_re, w_im)
            shift *= 2
        size = jnp.exp(rate_c * (lane + 1).astype(F32) + sums)
        cum_r[g], cum_i[g] = size * p_re, size * p_im
        last = lane == tok - 1
        h_re = to_row(jnp.sum(jnp.where(last, s_re, 0.0), axis=1, keepdims=True))
        h_im = to_row(jnp.sum(jnp.where(last, s_im, 0.0), axis=1, keepdims=True))
        end = jnp.sum(jnp.where(lane_g[row] == tok - 1, sums, 0.0), axis=1, keepdims=True)
        msg[g:g + 1, 0:states] = h_re
        msg[g:g + 1, states:2 * states] = jnp.broadcast_to(end, (1, states))
        msg[groups + g:groups + g + 1, 0:states] = h_im
        msg[groups + g:groups + g + 1, states:2 * states] = jnp.zeros((1, states), F32)
        loc_r[g] = (
            jnp.dot(cin_ref[g], s_re, precision=HIGH, preferred_element_type=F32)
            - jnp.dot(cq_ref[g], s_im, precision=HIGH, preferred_element_type=F32)
            + to_col(bypass[:, g * lanes:(g + 1) * lanes]) * u)

    mark("barrier")
    pl.semaphore_wait(barrier, n_sp - 1 + n_tp - 1)

    def send_head(k):
        return remote(msg, heads.at[me], s_pre.at[k], r_pre.at[me], k, mt)

    def head_from(k):
        return remote(msg, heads.at[k], s_pre.at[k], r_pre.at[k], me, mt)

    mark("send_head")
    span(me + 1, n_sp, lambda k: send_head(k).start())

    def columns_of(k):
        return pl.ds(pl.multiple_of(k * d_local, d_local), d_local)

    def send_wx(k):
        return remote(
            wexit_hbm.at[quarter, columns_of(k)], wx.at[mt, quarter, :],
            s_wx, r_wx.at[mt], me, k)

    def quarter_of(j):
        other = (x_part + j) % X_CHIPS
        rows = pl.ds(pl.multiple_of(other * part, part), part)
        return me - x_part + other, wx.at[:, rows, :], other

    def send_quarter(j):
        there, _, _ = quarter_of(j)
        mine = wx.at[:, quarter, :]
        return remote(mine, mine, s_wq, r_wq.at[x_part], there, mt)

    def send_dw(k):
        return remote(
            down_hbm.at[0, :, columns_of(k)], dw.at[mt], s_dw, r_dw.at[mt], me, k)

    def send_piece(d, c, k):
        there = chip(d) * CORES + c
        rows = pl.ds(k * PIECE, PIECE)
        return remote(
            down_hbm.at[0, rows, columns_of(there)], dw.at[mt, rows, :],
            s_dw, r_dw.at[mt], me, there)

    targets = [(d, c) for d in away for c in range(CORES)]

    def send_dw_to(those):
        for d, c in those:
            send_dw(chip(d) * CORES + c).start()

    mark("send_wx")
    each(n_tp, mt, lambda k: send_wx(k).start())
    send_dw_to(targets[:DW_EARLY])

    mark("routing")
    sel, score = sel_ref[...].astype(F32), score_ref[...]
    expert = iota((tok, n_sp), 1).astype(F32)
    hit0 = (to_col(sel[0:1]) == expert).astype(F32)
    hit1 = (to_col(sel[1:2]) == expert).astype(F32)
    hits = (hit0 + hit1).astype(BF16)
    below = (iota((tok, tok), 1) < iota((tok, tok), 0)).astype(F32).astype(BF16)
    rank = jnp.dot(below, hits, preferred_element_type=F32).astype(BF16)
    slot_e, slot_j = iota((n_sp, slots), 0), iota((n_sp, slots), 1)
    spread = ((slot_j >= slot_e * cap) & (slot_j < (slot_e + 1) * cap)).astype(F32).astype(BF16)
    hits_x = jnp.dot(hits, spread, preferred_element_type=F32)
    hit0_x = jnp.dot(hit0.astype(BF16), spread, preferred_element_type=F32)
    rank_x = jnp.dot(rank, spread, preferred_element_type=F32)
    place = jnp.bitwise_and(iota((tok, slots), 1), cap - 1).astype(F32)
    picked = (hits_x > 0.5) & (rank_x == place)
    disp[...] = picked.astype(F32).astype(BF16)
    both = score[0:1] + score[1:2]
    share = jnp.where(hit0_x > 0.5, to_col(score[0:1] / both), to_col(score[1:2] / both))
    share = jnp.where(picked, share, 0.0)
    high = share.astype(BF16)
    whi[...] = high
    wlo[...] = (share - high.astype(F32)).astype(BF16)

    mark("wait_head")
    span(0, me, lambda k: head_from(k).wait_recv())
    mark("enter")
    w_re, w_im = cos, sin
    shift = 1
    while shift < tok:
        w_re, w_im = times(w_re, w_im, w_re, w_im)
        shift *= 2
    in_re, in_im = jnp.zeros_like(rate), jnp.zeros_like(rate)
    for k in range(n_sp - 1):
        head = heads[k]
        size = jnp.exp(rate * float(tok) + head[0:groups, states:2 * states])
        n_re, n_im = times(size * w_re, size * w_im, in_re, in_im)
        n_re = n_re + head[0:groups, 0:states]
        n_im = n_im + head[groups:2 * groups, 0:states]
        in_re = jnp.where(k < me, n_re, in_re)
        in_im = jnp.where(k < me, n_im, in_im)
    for g in range(groups):
        row = slice(g, g + 1)
        c_re, c_im = times(cin_ref[g], cq_ref[g], in_re[row], in_im[row])
        value = (
            loc_r[g]
            + jnp.dot(c_re, cum_r[g], precision=HIGH, preferred_element_type=F32)
            - jnp.dot(c_im, cum_i[g], precision=HIGH, preferred_element_type=F32))
        mx[mt, g * lanes:(g + 1) * lanes, :] = jax.nn.gelu(value).astype(BF16)

    def send_mx(owner, tp):
        return remote(mx.at[owner], mx.at[owner], s_mx, r_mx.at[owner], me, tp)

    mark("send_mx")
    for d in away:
        send_mx(mt, chip(d) * CORES + core).start()
    send_mx(mt, twin).start()

    def got(dst, sem):
        remote(dst, dst, s_mx, sem, me, twin).wait_recv()

    mark("wait_quarter")
    local[2].wait()
    each(n_tp, mt, lambda k: got(wx.at[k, quarter, :], r_wx.at[k]))
    for j in range(1, X_CHIPS):
        send_quarter(j).start()
    send_dw_to(targets[DW_EARLY:DW_MID])
    send_dw(twin).start()

    mark("relay_mx")
    local[0].wait()
    for d in away:
        owner = chip(-d) * CORES + core
        got(mx.at[owner], r_mx.at[owner])
        send_mx(owner, twin).start()
    mark("wait_wq")
    for j in range(1, X_CHIPS):
        _, dst, other = quarter_of(j)
        got(dst, r_wq.at[other])
    mark("wait_mx")
    for d in [0] + away:
        owner = chip(-d) * CORES + (1 - core)
        got(mx.at[owner], r_mx.at[owner])
    mark("project")
    projected = lax.dot_general(
        mx[...].reshape(n_tp * chan, tok), wx[...].reshape(n_tp * chan, d_local),
        (((0,), (0,)), ((), ())), preferred_element_type=F32).astype(BF16)
    stream = (skip[...].astype(F32) + projected.astype(F32)).astype(BF16)
    stream_f = stream.astype(F32)
    stream_s[...] = stream_f

    sent = lax.dot_general(
        disp[...], stream, (((0,), (0,)), ((), ())),
        preferred_element_type=F32).astype(BF16).reshape(n_sp, cap, d_local)
    xs[...] = sent

    def rows_of(k):
        start = k * cap
        return pl.ds(start if isinstance(k, int) else pl.multiple_of(start, cap), cap)

    own_place = n_sp - 1

    def send_rows(dz, dx):
        k, place = at_offset(dz, dx), place_at(dz, dx)
        return remote(
            xs.at[k], g_buf.at[mt, rows_of(place), :], s_dis, r_dis.at[place], k, mt)

    mark("send_rows")
    far_first(lambda dz, dx: send_rows(dz, dx).start())
    own_rows = pltpu.make_async_copy(
        xs.at[me], g_buf.at[mt, rows_of(own_place), :], l_sem.at[6])
    own_rows.start()

    deepest = n_y // 2

    way = 1 - 2 * core
    onward = around(y + way, n_y) * CORES + core

    def rows_in(q):
        return pl.ds(q * rows_q, rows_q)

    def half_in(q, side):
        size = rows_q // CORES
        return pl.ds(pl.multiple_of(q * rows_q + side * size, size), size)

    def chip_rows(buf, there, rows):
        return buf.at[pl.ds(there * CORES, CORES), rows, :]

    def ring_hop(buf, sems, q, h):
        send, one, ring, handed = sems

        def push(view, sem, tp):
            remote(view, view, send.at[q], sem, me, tp).start()

        if h == 0:
            for tp in (chip(1) * CORES, chip(-1) * CORES + 1, twin):
                push(buf.at[mt, rows_in(q), :], one.at[mt, q], tp)
            return
        there = around(y - way * h, n_y)
        view = chip_rows(buf, there, rows_in(q) if h < deepest else half_in(q, core))
        if h == 1:
            for c in range(CORES):
                owner = there * CORES + c
                got(buf.at[owner, rows_in(q), :], one.at[owner, q])
        else:
            got(view, ring.at[there, q])
        if h < deepest:
            rows = rows_in(q) if h < deepest - 1 else half_in(q, core)
            push(chip_rows(buf, there, rows), ring.at[there, q], onward)
        push(view, handed.at[there, q], twin)

    def normed(both, there, rows, fresh):
        depth = CORES * d_local
        full = both.astype(F32)
        square = full * full
        total = square[:, 0:128]
        for k in range(1, depth // 128):
            total = total + square[:, k * 128:(k + 1) * 128]
        squares[rows, :] = total if fresh else squares[rows, :] + total
        gains = gain[:, pl.ds(pl.multiple_of(there * depth, depth), depth)]
        return (full * gains).astype(BF16)

    def pairs(buf, sems, q, h, weights, target, need=None):
        _, one, _, handed = sems
        rows = rows_in(q)

        def multiply(there):
            both = jnp.concatenate(
                [buf[there * CORES, rows, :], buf[there * CORES + 1, rows, :]], axis=1)
            if need is None:
                both = normed(both, there, rows, h == 0)
            part = jnp.dot(both, weights(there), preferred_element_type=F32)
            if h == 0:
                target[rows, :] = part
            else:
                target[rows, :] += part

        if need is not None:
            need(h)
        other = around(y + way * h, n_y)
        if h == 0:
            got(buf.at[twin, rows, :], one.at[twin, q])
        elif h < deepest:
            multiply(around(y - way * h, n_y))
            got(chip_rows(buf, other, rows), handed.at[other, q])
        else:
            got(chip_rows(buf, other, half_in(q, 1 - core)), handed.at[other, q])
        multiply(other)

    def gate_up(there):
        depth = CORES * d_local
        return gu[pl.ds(pl.multiple_of(there * depth, depth), depth), :]

    def down_here(k):
        if k == 0:
            local[5].wait()
            got(dw.at[twin], r_dw.at[twin])
        else:
            for d in (k, -k) if 2 * k < n_y else (k,):
                for c in range(CORES):
                    owner = chip(d) * CORES + c
                    got(dw.at[owner], r_dw.at[owner])

    def down(there):
        return jnp.concatenate([dw[there * CORES], dw[there * CORES + 1]], axis=0)

    def send_back(place):
        k = at_offset(*near[place])
        return remote(
            outb.at[rows_of(place), :], ret.at[rows_of(me), :], s_ret, r_ret.at[me], k, mt)

    own_back = pltpu.make_async_copy(
        outb.at[rows_of(own_place), :], ret.at[rows_of(me), :], l_sem.at[7])

    seen = set()
    g_sems, h_sems = ring_sems[:4], ring_sems[4:]

    def stage(r, q, st):
        rows = slice(q * rows_q, (q + 1) * rows_q)
        first = deepest + 1

        def need(k):
            if k not in seen:
                seen.add(k)
                down_here(k)

        if st == 0:
            for place in range(q * sp_q, (q + 1) * sp_q):
                if place == own_place:
                    own_rows.wait()
                else:
                    got(g_buf.at[mt, rows_of(place), :], r_dis.at[place])
            ring_hop(g_buf, g_sems, q, 0)
        elif st <= deepest:
            ring_hop(g_buf, g_sems, q, st)
            pairs(g_buf, g_sems, q, st - 1, gate_up, acc)
        elif st == first:
            pairs(g_buf, g_sems, q, deepest, gate_up, acc)
            mean = jnp.sum(squares[rows, :], axis=1, keepdims=True) * (1.0 / width)
            factor = lax.rsqrt(mean + EPS)
            gate = acc[rows, 0:f_local] * factor
            wide = acc[rows, f_local:2 * f_local] * factor
            h_buf[mt, rows, :] = (jax.nn.silu(gate) * wide).astype(BF16)
            ring_hop(h_buf, h_sems, q, 0)
        elif st <= first + deepest:
            ring_hop(h_buf, h_sems, q, st - first)
            pairs(h_buf, h_sems, q, st - first - 1, down, oacc, need)
        else:
            pairs(h_buf, h_sems, q, deepest, down, oacc, need)
            outb[rows, :] = oacc[rows, :].astype(BF16)

            for place in range(q * sp_q, (q + 1) * sp_q):
                if place == own_place:
                    own_back.start()
                else:
                    send_back(place).start()

    last_stage = 2 * deepest + 2
    pieces = [
        (d, c, k) for d, c in targets[DW_MID:] for k in range(f_local // PIECE)]
    order = sorted(
        (st + SKEW * r if st else -1, r, q, st)
        for r, q in enumerate(CHUNK_ORDER) for st in range(last_stage + 1))
    for now, (_, r, q, st) in enumerate(order):
        if st == 1 and r == 0:
            mark("wait_small")
            local[1].wait()
            local[3].wait()
            local[4].wait()
            span(me + 1, n_sp, lambda k: send_head(k).wait_send())
        mark(f"stage#n={now}#r={r}#st={st}")
        stage(r, q, st)
        for d, c, k in pieces[:DW_SLOTS.count((r, st))]:
            send_piece(d, c, k).start()
        del pieces[:DW_SLOTS.count((r, st))]

    assert not pieces
    mark("wait_back")
    own_back.wait()
    each(n_sp, me, lambda k: got(ret.at[rows_of(k), :], r_ret.at[k]))
    mark("combine")
    back = ret[...]
    out_ref[...] = (
        stream_s[...]
        + jnp.dot(whi[...], back, preferred_element_type=F32)
        + jnp.dot(wlo[...], back, preferred_element_type=F32)).astype(BF16)

    mark("drain")

    def sent_all(view, sem):
        remote(view, view, sem, sem, me, twin).wait_send()

    sent_all(wx.at[pl.ds(0, n_tp - 1), quarter, :], s_wx)
    sent_all(wx.at[:, pl.ds(0, part * (X_CHIPS - 1)), :], s_wq)
    sent_all(mx.at[pl.ds(0, 2 * n_y - 1)], s_mx)
    sent_all(dw.at[pl.ds(0, n_tp - 1)], s_dw)
    sent_all(xs.at[pl.ds(0, n_sp - 1)], s_dis)
    sent_all(outb.at[pl.ds(0, (n_sp - 1) * cap), :], s_ret)
    for q in range(CHUNKS):
        rows = pl.ds(q * rows_q, rows_q)
        sent_all(g_buf.at[pl.ds(0, 2 * n_y - 1), rows, :], g_sems[0].at[q])
        sent_all(h_buf.at[pl.ds(0, 2 * n_y - 1), rows, :], h_sems[0].at[q])
    mark(None)


def per_device(
    lane_source_signal, spectral_damping_part, spectral_angular_part, interval_exponent,
    entry_matrix_inphase, entry_matrix_quadrature, emission_inphase, emission_quadrature,
    lane_bypass_factor, spike_shrink_offset, lane_exit_matrix, skipline_stream,
    specialist_scaling_vector, selected_specialists, dispatcher_scores,
    specialist_valve_matrix, specialist_widen_matrix, specialist_shrink_matrix,
):
    n_sp, n_tp = lax.axis_size("sp"), lax.axis_size("tp")
    groups, states, lanes = entry_matrix_inphase.shape
    chan, tok = lane_source_signal.shape
    width = specialist_scaling_vector.shape[0]
    d_local = width // n_tp
    f_local = specialist_valve_matrix.shape[2]
    cap = 2 * tok * selected_specialists.shape[1] // n_sp
    slots = n_sp * cap
    dims = (n_sp, n_tp, groups, states, lanes, tok, width, cap)
    vmem = pl.BlockSpec(memory_space=pltpu.VMEM)
    operands = (
        lane_source_signal, spectral_damping_part, spectral_angular_part,
        interval_exponent.reshape(1, groups), entry_matrix_inphase.transpose(0, 2, 1),
        entry_matrix_quadrature.transpose(0, 2, 1),
        emission_inphase, emission_quadrature, lane_bypass_factor.reshape(1, chan),
        spike_shrink_offset, selected_specialists.T, dispatcher_scores.T, lane_exit_matrix,
        skipline_stream, specialist_scaling_vector.reshape(1, width),
        specialist_valve_matrix, specialist_widen_matrix, specialist_shrink_matrix,
    )
    hbm = pl.BlockSpec(memory_space=pl.ANY)
    dma = pltpu.SemaphoreType.DMA
    scratch = [pltpu.VMEM(a.shape, a.dtype) for a in operands[:12]] + [
        pltpu.VMEM((8, 128), F32),
        pltpu.VMEM((n_sp, 8, 128), F32),
        pltpu.VMEM((n_tp, chan, d_local), BF16),
        pltpu.VMEM((n_tp, chan, tok), BF16),
        pltpu.VMEM((n_tp, f_local, d_local), BF16),
        pltpu.VMEM((width, 2 * f_local), BF16),
        pltpu.VMEM((tok, d_local), BF16),
        pltpu.VMEM((1, width), F32),
        pltpu.VMEM((slots, 128), F32),
        pltpu.VMEM((tok, slots), BF16),
        pltpu.VMEM((tok, slots), BF16),
        pltpu.VMEM((tok, slots), BF16),
        pltpu.VMEM((n_sp, cap, d_local), BF16),
        pltpu.VMEM((n_tp, slots, d_local), BF16),
        pltpu.VMEM((n_tp, slots, f_local), BF16),
        pltpu.VMEM((slots, 2 * f_local), F32),
        pltpu.VMEM((slots, d_local), F32),
        pltpu.VMEM((slots, d_local), BF16),
        pltpu.VMEM((slots, d_local), BF16),
        pltpu.VMEM((tok, d_local), F32),
        pltpu.VMEM((groups, lanes, tok), F32),
        pltpu.VMEM((groups, states, tok), F32),
        pltpu.VMEM((groups, states, tok), F32),
        dma((12,)), dma((8,)),
        dma((n_sp,)), dma((n_sp,)),
        dma, dma((n_tp,)), dma, dma((X_CHIPS,)), dma, dma((n_tp,)), dma, dma((n_tp,)),
        dma, dma((n_sp,)), dma, dma((n_sp,)),
    ] + 2 * [
        dma((CHUNKS,)), dma((n_tp, CHUNKS)),
        dma((n_tp // CORES, CHUNKS)), dma((n_tp // CORES, CHUNKS)),
    ]
    return pl.pallas_call(
        functools.partial(mixer_kernel, dims),
        out_shape=jax.ShapeDtypeStruct((tok, d_local), BF16),
        in_specs=[hbm] * 18,
        out_specs=vmem,
        scratch_shapes=scratch,
        compiler_params=pltpu.CompilerParams(
            collective_id=0, has_side_effects=True, vmem_limit_bytes=60 * 1024 * 1024),
    )(*operands)


def solution(mesh):
    placed = (
        P("tp", "sp"), P("tp", None), P("tp", None), P("tp"), P("tp", None, None),
        P("tp", None, None), P("tp", None, None), P("tp", None, None), P("tp"),
        P("tp", "sp"), P("tp", None), P("sp", None), P(), P("sp", None), P("sp", None),
        P("sp", None, "tp"), P("sp", None, "tp"), P("sp", "tp", None),
    )
    return jax.shard_map(
        per_device, mesh=mesh, in_specs=placed, out_specs=P("sp", "tp"), check_vma=False
    )
```

```python
import functools

import jax
import jax.numpy as jnp
from jax import lax
from jax.experimental import pallas as pl
from jax.experimental.pallas import tpu as pltpu
from jax.sharding import PartitionSpec as P

EPS = 1e-06
HIGH = lax.Precision.HIGHEST
MESH = pl.DeviceIdType.MESH
F32 = jnp.float32
BF16 = jnp.bfloat16
CORES = 2
CHUNKS = 4
SKEW = 0.5
X_CHIPS = 4
DW_EARLY, DW_MID = 4, 12
PIECE = 32
DW_SLOTS = ((2, 3), (3, 3), (0, 4), (1, 4), (2, 4), (3, 4), (0, 6), (1, 6))
GROUP_SETS = ((0, 1, 2, 3),)
CHUNK_ORDER = (0, 1, 2, 3)


def iota(shape, dim):
    return lax.broadcasted_iota(jnp.int32, shape, dim)


def to_col(row):
    n = row.shape[1]
    eye = iota((n, n), 0) == iota((n, n), 1)
    return jnp.sum(jnp.where(eye, row, 0.0), axis=1, keepdims=True)


def to_row(col):
    n = col.shape[0]
    eye = iota((n, n), 0) == iota((n, n), 1)
    return jnp.sum(jnp.where(eye, col, 0.0), axis=0, keepdims=True)


def small_expm1(x):
    total = jnp.ones_like(x)
    for k in range(11, 1, -1):
        total = 1.0 + total * x * (1.0 / k)
    return jnp.where(x > -0.7, x * total, jnp.exp(x) - 1.0)


def dot_first(a, b):
    return lax.dot_general(
        a, b, (((0,), (0,)), ((), ())), precision=HIGH, preferred_element_type=F32)


def times(ar, ai, br, bi):
    return ar * br - ai * bi, ar * bi + ai * br


def mixer_kernel(
    dims,
    u_hbm, damp_hbm, ang_hbm, ie_hbm, ein_hbm, eq_hbm, cin_hbm, cq_hbm, byp_hbm, off_hbm,
    sel_hbm, score_hbm, wexit_hbm, skip_hbm, gain_hbm, gate_hbm, up_hbm, down_hbm,
    out_ref,
    u_ref, damp_ref, ang_ref, ie_ref, ein_ref, eq_ref, cin_ref, cq_ref, byp_ref, off_ref,
    sel_ref, score_ref,
    msg, heads, wx, mx, dw, gu, skip, gain, squares, disp, whi, wlo,
    xs, g_buf, h_buf, acc, oacc, outb, ret, stream_s, loc_r, cum_r, cum_i,
    i_sem, l_sem, s_pre, r_pre, s_wx, r_wx, s_wq, r_wq, s_mx, r_mx, s_dw, r_dw,
    s_dis, r_dis, s_ret, r_ret, *ring_sems,
):
    n_sp, n_tp, groups, states, lanes, tok, width, cap = dims
    n_y = n_tp // CORES
    d_local = width // n_tp
    f_local = gate_hbm.shape[2]
    slots = n_sp * cap
    rows_q = slots // CHUNKS
    sp_q = n_sp // CHUNKS
    me, mt = lax.axis_index("sp"), lax.axis_index("tp")
    y, core = mt // CORES, mt % CORES
    twin = y * CORES + (1 - core)
    x_part = me % X_CHIPS
    away = [k for d in range(1, n_y // 2 + 1) for k in ((d, -d) if 2 * d < n_y else (d,))]

    def chip(k):
        return around(y + k, n_y)

    def around(value, count):
        if count & (count - 1):
            return lax.rem(value + count, count)
        return jnp.bitwise_and(value, count - 1)

    def each(count, mine, fn):
        for j in range(1, count):
            fn(around(mine + j, count))

    n_z = n_sp // X_CHIPS
    near = sorted(
        ((dz, dx) for dz in range(-((n_z - 1) // 2), n_z // 2 + 1)
         for dx in range(-((X_CHIPS - 1) // 2), X_CHIPS // 2 + 1)),
        key=lambda o: (-(abs(o[0]) + abs(o[1])), -abs(o[0]), o))

    def at_offset(dz, dx):
        return around(me // X_CHIPS + dz, n_z) * X_CHIPS + around(x_part + dx, X_CHIPS)

    def place_at(dz, dx):
        back = [
            k for k, (a, b) in enumerate(near)
            if (a + dz) % n_z == 0 and (b + dx) % X_CHIPS == 0]
        return back[0]

    def far_first(fn):
        for dz, dx in near[:-1]:
            fn(dz, dx)

    def span(lo, hi, fn):
        def step(j, carry):
            fn(j)
            return carry
        lax.fori_loop(lo, hi, step, 0)

    def remote(src, dst, send, recv, sp, tp):
        return pltpu.make_async_remote_copy(
            src_ref=src, dst_ref=dst, send_sem=send, recv_sem=recv,
            device_id=(sp, tp), device_id_type=MESH)

    scope = []

    def mark(name):
        if scope:
            scope.pop().__exit__(None, None, None)
        if name:
            scope.append(jax.named_scope(name))
            scope[-1].__enter__()

    heads[...] = jnp.zeros_like(heads)
    barrier = pltpu.get_barrier_semaphore()
    far_first(lambda dz, dx: pl.semaphore_signal(
        barrier, inc=1, device_id=(at_offset(dz, dx), mt), device_id_type=MESH))
    for d in away[::-1]:
        for c in range(CORES):
            pl.semaphore_signal(
                barrier, inc=1, device_id=(me, chip(d) * CORES + c), device_id_type=MESH)
    pl.semaphore_signal(barrier, inc=1, device_id=(me, twin), device_id_type=MESH)

    small = [
        pltpu.make_async_copy(src, dst, i_sem.at[k])
        for k, (src, dst) in enumerate((
            (ie_hbm, ie_ref), (damp_hbm, damp_ref), (ang_hbm, ang_ref), (off_hbm, off_ref),
            (u_hbm, u_ref), (ein_hbm, ein_ref), (eq_hbm, eq_ref), (cin_hbm, cin_ref),
            (cq_hbm, cq_ref), (byp_hbm, byp_ref), (sel_hbm, sel_ref), (score_hbm, score_ref)))
    ]
    for copy in small:
        copy.start()

    mark("local_copies")
    own_cols = pl.ds(pl.multiple_of(mt * d_local, d_local), d_local)
    chan = groups * lanes
    part = chan // X_CHIPS
    quarter = pl.ds(pl.multiple_of(x_part * part, part), part)
    local = [
        pltpu.make_async_copy(skip_hbm.at[:, own_cols], skip, l_sem.at[0]),
        pltpu.make_async_copy(gain_hbm, gain, l_sem.at[1]),
        pltpu.make_async_copy(
            wexit_hbm.at[quarter, own_cols], wx.at[mt, quarter, :], l_sem.at[2]),
        pltpu.make_async_copy(gate_hbm.at[0], gu.at[:, pl.ds(0, f_local)], l_sem.at[3]),
        pltpu.make_async_copy(up_hbm.at[0], gu.at[:, pl.ds(f_local, f_local)], l_sem.at[4]),
        pltpu.make_async_copy(down_hbm.at[0, :, own_cols], dw.at[mt], l_sem.at[5]),
    ]
    for copy in local:
        copy.start()

    mark("state")
    for copy in small:
        copy.wait()
    step_size = jnp.exp(to_col(ie_ref[...]))
    damp, ang = damp_ref[...], ang_ref[...]
    rate, angle = damp * step_size, ang * step_size
    cos, sin = jnp.cos(angle), jnp.sin(angle)
    half = jnp.sin(0.5 * angle)
    num_re = small_expm1(rate) * cos - 2.0 * half * half
    num_im = jnp.exp(rate) * sin
    denom = damp * damp + ang * ang
    fac_re = (num_re * damp + num_im * ang) / denom
    fac_im = (num_im * damp - num_re * ang) / denom
    total = off_ref[...]
    lane_g = iota(total.shape, 1)
    shift = 1
    while shift < tok:
        total = total + jnp.where(lane_g >= shift, pltpu.roll(total, shift, 1), 0.0)
        shift *= 2
    lane = iota((states, tok), 1)
    bypass = byp_ref[...]
    each_group = range(groups)
    rows_g = [slice(g, g + 1) for g in each_group]
    signal = [u_ref[g * lanes:(g + 1) * lanes, :].astype(F32) for g in each_group]
    e_re = [dot_first(ein_ref[g], signal[g]) for g in each_group]
    e_im = [dot_first(eq_ref[g], signal[g]) for g in each_group]
    rate_c = [to_col(rate[row]) for row in rows_g]
    w = [(to_col(cos[row]), to_col(sin[row])) for row in rows_g]
    s = [
        times(to_col(fac_re[row]), to_col(fac_im[row]), e_re[g], e_im[g])
        for g, row in enumerate(rows_g)]
    p = [(jnp.ones((states, tok), F32), jnp.zeros((states, tok), F32))] * groups
    for pair in GROUP_SETS:
        shift = 1
        while shift <= tok:
            taken = (jnp.bitwise_and(lane + 1, shift)) != 0
            for g in pair:
                sums = total[rows_g[g]]
                q_re, q_im = times(*p[g], *w[g])
                p[g] = jnp.where(taken, q_re, p[g][0]), jnp.where(taken, q_im, p[g][1])
                if shift < tok:
                    gap = sums - pltpu.roll(sums, shift, 1)
                    size = jnp.exp(rate_c[g] * float(shift) + jnp.minimum(gap, 0.0))
                    size = jnp.where(lane >= shift, size, 0.0)
                    t_re, t_im = times(
                        *w[g], pltpu.roll(s[g][0], shift, 1), pltpu.roll(s[g][1], shift, 1))
                    s[g] = s[g][0] + size * t_re, s[g][1] + size * t_im
                    w[g] = times(*w[g], *w[g])
            shift *= 2
        for g in pair:
            size = jnp.exp(rate_c[g] * (lane + 1).astype(F32) + total[rows_g[g]])
            cum_r[g], cum_i[g] = size * p[g][0], size * p[g][1]
    last = lane == tok - 1
    for g, row in enumerate(rows_g):
        h_re = to_row(jnp.sum(jnp.where(last, s[g][0], 0.0), axis=1, keepdims=True))
        h_im = to_row(jnp.sum(jnp.where(last, s[g][1], 0.0), axis=1, keepdims=True))
        end = jnp.sum(
            jnp.where(lane_g[row] == tok - 1, total[row], 0.0), axis=1, keepdims=True)
        msg[g:g + 1, 0:states] = h_re
        msg[g:g + 1, states:2 * states] = jnp.broadcast_to(end, (1, states))
        msg[groups + g:groups + g + 1, 0:states] = h_im
        msg[groups + g:groups + g + 1, states:2 * states] = jnp.zeros((1, states), F32)
        loc_r[g] = (
            jnp.dot(cin_ref[g], s[g][0], precision=HIGH, preferred_element_type=F32)
            - jnp.dot(cq_ref[g], s[g][1], precision=HIGH, preferred_element_type=F32)
            + to_col(bypass[:, g * lanes:(g + 1) * lanes]) * signal[g])

    mark("barrier")
    pl.semaphore_wait(barrier, n_sp - 1 + n_tp - 1)

    def send_head(k):
        return remote(msg, heads.at[me], s_pre.at[k], r_pre.at[me], k, mt)

    def head_from(k):
        return remote(msg, heads.at[k], s_pre.at[k], r_pre.at[k], me, mt)

    mark("send_head")
    span(me + 1, n_sp, lambda k: send_head(k).start())

    def columns_of(k):
        return pl.ds(pl.multiple_of(k * d_local, d_local), d_local)

    def send_wx(k):
        return remote(
            wexit_hbm.at[quarter, columns_of(k)], wx.at[mt, quarter, :],
            s_wx, r_wx.at[mt], me, k)

    def quarter_of(j):
        other = (x_part + j) % X_CHIPS
        rows = pl.ds(pl.multiple_of(other * part, part), part)
        return me - x_part + other, wx.at[:, rows, :], other

    def send_quarter(j):
        there, _, _ = quarter_of(j)
        mine = wx.at[:, quarter, :]
        return remote(mine, mine, s_wq, r_wq.at[x_part], there, mt)

    def send_dw(k):
        return remote(
            down_hbm.at[0, :, columns_of(k)], dw.at[mt], s_dw, r_dw.at[mt], me, k)

    def send_piece(d, c, k):
        there = chip(d) * CORES + c
        rows = pl.ds(k * PIECE, PIECE)
        return remote(
            down_hbm.at[0, rows, columns_of(there)], dw.at[mt, rows, :],
            s_dw, r_dw.at[mt], me, there)

    targets = [(d, c) for d in away for c in range(CORES)]

    def send_dw_to(those):
        for d, c in those:
            send_dw(chip(d) * CORES + c).start()

    mark("send_wx")
    each(n_tp, mt, lambda k: send_wx(k).start())
    send_dw_to(targets[:DW_EARLY])

    mark("routing")
    sel, score = sel_ref[...].astype(F32), score_ref[...]
    expert = iota((tok, n_sp), 1).astype(F32)
    hit0 = (to_col(sel[0:1]) == expert).astype(F32)
    hit1 = (to_col(sel[1:2]) == expert).astype(F32)
    hits = (hit0 + hit1).astype(BF16)
    below = (iota((tok, tok), 1) < iota((tok, tok), 0)).astype(F32).astype(BF16)
    rank = jnp.dot(below, hits, preferred_element_type=F32).astype(BF16)
    slot_e, slot_j = iota((n_sp, slots), 0), iota((n_sp, slots), 1)
    spread = ((slot_j >= slot_e * cap) & (slot_j < (slot_e + 1) * cap)).astype(F32).astype(BF16)
    hits_x = jnp.dot(hits, spread, preferred_element_type=F32)
    hit0_x = jnp.dot(hit0.astype(BF16), spread, preferred_element_type=F32)
    rank_x = jnp.dot(rank, spread, preferred_element_type=F32)
    place = jnp.bitwise_and(iota((tok, slots), 1), cap - 1).astype(F32)
    picked = (hits_x > 0.5) & (rank_x == place)
    disp[...] = picked.astype(F32).astype(BF16)
    both = score[0:1] + score[1:2]
    share = jnp.where(hit0_x > 0.5, to_col(score[0:1] / both), to_col(score[1:2] / both))
    share = jnp.where(picked, share, 0.0)
    high = share.astype(BF16)
    whi[...] = high
    wlo[...] = (share - high.astype(F32)).astype(BF16)

    mark("wait_head")
    span(0, me, lambda k: head_from(k).wait_recv())
    mark("enter")
    w_re, w_im = cos, sin
    shift = 1
    while shift < tok:
        w_re, w_im = times(w_re, w_im, w_re, w_im)
        shift *= 2
    in_re, in_im = jnp.zeros_like(rate), jnp.zeros_like(rate)
    for k in range(n_sp - 1):
        head = heads[k]
        size = jnp.exp(rate * float(tok) + head[0:groups, states:2 * states])
        n_re, n_im = times(size * w_re, size * w_im, in_re, in_im)
        n_re = n_re + head[0:groups, 0:states]
        n_im = n_im + head[groups:2 * groups, 0:states]
        in_re = jnp.where(k < me, n_re, in_re)
        in_im = jnp.where(k < me, n_im, in_im)
    for g in range(groups):
        row = slice(g, g + 1)
        c_re, c_im = times(cin_ref[g], cq_ref[g], in_re[row], in_im[row])
        value = (
            loc_r[g]
            + jnp.dot(c_re, cum_r[g], precision=HIGH, preferred_element_type=F32)
            - jnp.dot(c_im, cum_i[g], precision=HIGH, preferred_element_type=F32))
        mx[mt, g * lanes:(g + 1) * lanes, :] = jax.nn.gelu(value).astype(BF16)

    def send_mx(owner, tp):
        return remote(mx.at[owner], mx.at[owner], s_mx, r_mx.at[owner], me, tp)

    mark("send_mx")
    for d in away:
        send_mx(mt, chip(d) * CORES + core).start()
    send_mx(mt, twin).start()

    def got(dst, sem):
        remote(dst, dst, s_mx, sem, me, twin).wait_recv()

    mark("wait_quarter")
    local[2].wait()
    each(n_tp, mt, lambda k: got(wx.at[k, quarter, :], r_wx.at[k]))
    for j in (2, 1, 3):
        send_quarter(j).start()
    send_dw_to(targets[DW_EARLY:DW_MID])
    send_dw(twin).start()

    mark("relay_mx")
    local[0].wait()
    for d in away:
        owner = chip(-d) * CORES + core
        got(mx.at[owner], r_mx.at[owner])
        send_mx(owner, twin).start()
    mark("wait_wq")
    for j in range(1, X_CHIPS):
        _, dst, other = quarter_of(j)
        got(dst, r_wq.at[other])
    mark("wait_mx")
    for d in [0] + away:
        owner = chip(-d) * CORES + (1 - core)
        got(mx.at[owner], r_mx.at[owner])
    mark("project")
    projected = lax.dot_general(
        mx[...].reshape(n_tp * chan, tok), wx[...].reshape(n_tp * chan, d_local),
        (((0,), (0,)), ((), ())), preferred_element_type=F32).astype(BF16)
    stream = (skip[...].astype(F32) + projected.astype(F32)).astype(BF16)
    stream_f = stream.astype(F32)
    stream_s[...] = stream_f

    sent = lax.dot_general(
        disp[...], stream, (((0,), (0,)), ((), ())),
        preferred_element_type=F32).astype(BF16).reshape(n_sp, cap, d_local)
    xs[...] = sent

    def rows_of(k):
        start = k * cap
        return pl.ds(start if isinstance(k, int) else pl.multiple_of(start, cap), cap)

    own_place = n_sp - 1

    def send_rows(dz, dx):
        k, place = at_offset(dz, dx), place_at(dz, dx)
        return remote(
            xs.at[k], g_buf.at[mt, rows_of(place), :], s_dis, r_dis.at[place], k, mt)

    mark("send_rows")
    far_first(lambda dz, dx: send_rows(dz, dx).start())
    own_rows = pltpu.make_async_copy(
        xs.at[me], g_buf.at[mt, rows_of(own_place), :], l_sem.at[6])
    own_rows.start()

    deepest = n_y // 2

    way = 1 - 2 * core
    onward = around(y + way, n_y) * CORES + core

    def rows_in(q):
        return pl.ds(q * rows_q, rows_q)

    def half_in(q, side):
        size = rows_q // CORES
        return pl.ds(pl.multiple_of(q * rows_q + side * size, size), size)

    def chip_rows(buf, there, rows):
        return buf.at[pl.ds(there * CORES, CORES), rows, :]

    def ring_hop(buf, sems, q, h):
        send, one, ring, handed = sems

        def push(view, sem, tp):
            remote(view, view, send.at[q], sem, me, tp).start()

        if h == 0:
            for tp in (chip(1) * CORES, chip(-1) * CORES + 1, twin):
                push(buf.at[mt, rows_in(q), :], one.at[mt, q], tp)
            return
        there = around(y - way * h, n_y)
        view = chip_rows(buf, there, rows_in(q) if h < deepest else half_in(q, core))
        if h == 1:
            for c in range(CORES):
                owner = there * CORES + c
                got(buf.at[owner, rows_in(q), :], one.at[owner, q])
        else:
            got(view, ring.at[there, q])
        if h < deepest:
            rows = rows_in(q) if h < deepest - 1 else half_in(q, core)
            push(chip_rows(buf, there, rows), ring.at[there, q], onward)
        push(view, handed.at[there, q], twin)

    def normed(both, there, rows, fresh):
        depth = CORES * d_local
        full = both.astype(F32)
        square = full * full
        total = square[:, 0:128]
        for k in range(1, depth // 128):
            total = total + square[:, k * 128:(k + 1) * 128]
        squares[rows, :] = total if fresh else squares[rows, :] + total
        gains = gain[:, pl.ds(pl.multiple_of(there * depth, depth), depth)]
        return (full * gains).astype(BF16)

    def pairs(buf, sems, q, h, weights, target, need=None):
        _, one, _, handed = sems
        rows = rows_in(q)

        def multiply(there):
            both = jnp.concatenate(
                [buf[there * CORES, rows, :], buf[there * CORES + 1, rows, :]], axis=1)
            if need is None:
                both = normed(both, there, rows, h == 0)
            part = jnp.dot(both, weights(there), preferred_element_type=F32)
            if h == 0:
                target[rows, :] = part
            else:
                target[rows, :] += part

        if need is not None:
            need(h)
        other = around(y + way * h, n_y)
        if h == 0:
            got(buf.at[twin, rows, :], one.at[twin, q])
        elif h < deepest:
            multiply(around(y - way * h, n_y))
            got(chip_rows(buf, other, rows), handed.at[other, q])
        else:
            got(chip_rows(buf, other, half_in(q, 1 - core)), handed.at[other, q])
        multiply(other)

    def gate_up(there):
        depth = CORES * d_local
        return gu[pl.ds(pl.multiple_of(there * depth, depth), depth), :]

    def down_here(k):
        if k == 0:
            local[5].wait()
            got(dw.at[twin], r_dw.at[twin])
        else:
            for d in (k, -k) if 2 * k < n_y else (k,):
                for c in range(CORES):
                    owner = chip(d) * CORES + c
                    got(dw.at[owner], r_dw.at[owner])

    def down(there):
        return jnp.concatenate([dw[there * CORES], dw[there * CORES + 1]], axis=0)

    def send_back(place):
        k = at_offset(*near[place])
        return remote(
            outb.at[rows_of(place), :], ret.at[rows_of(me), :], s_ret, r_ret.at[me], k, mt)

    own_back = pltpu.make_async_copy(
        outb.at[rows_of(own_place), :], ret.at[rows_of(me), :], l_sem.at[7])

    seen = set()
    g_sems, h_sems = ring_sems[:4], ring_sems[4:]

    def stage(r, q, st):
        rows = slice(q * rows_q, (q + 1) * rows_q)
        first = deepest + 1

        def need(k):
            if k not in seen:
                seen.add(k)
                down_here(k)

        if st == 0:
            for place in range(q * sp_q, (q + 1) * sp_q):
                if place == own_place:
                    own_rows.wait()
                else:
                    got(g_buf.at[mt, rows_of(place), :], r_dis.at[place])
            ring_hop(g_buf, g_sems, q, 0)
        elif st <= deepest:
            ring_hop(g_buf, g_sems, q, st)
            pairs(g_buf, g_sems, q, st - 1, gate_up, acc)
        elif st == first:
            pairs(g_buf, g_sems, q, deepest, gate_up, acc)
            mean = jnp.sum(squares[rows, :], axis=1, keepdims=True) * (1.0 / width)
            factor = lax.rsqrt(mean + EPS)
            gate = acc[rows, 0:f_local] * factor
            wide = acc[rows, f_local:2 * f_local] * factor
            h_buf[mt, rows, :] = (jax.nn.silu(gate) * wide).astype(BF16)
            ring_hop(h_buf, h_sems, q, 0)
        elif st <= first + deepest:
            ring_hop(h_buf, h_sems, q, st - first)
            pairs(h_buf, h_sems, q, st - first - 1, down, oacc, need)
        else:
            pairs(h_buf, h_sems, q, deepest, down, oacc, need)
            outb[rows, :] = oacc[rows, :].astype(BF16)

            for place in range(q * sp_q, (q + 1) * sp_q):
                if place == own_place:
                    own_back.start()
                else:
                    send_back(place).start()

    last_stage = 2 * deepest + 2
    pieces = [
        (d, c, k) for d, c in targets[DW_MID:] for k in range(f_local // PIECE)]
    order = sorted(
        (st + SKEW * r if st else -1, r, q, st)
        for r, q in enumerate(CHUNK_ORDER) for st in range(last_stage + 1))
    for now, (_, r, q, st) in enumerate(order):
        if st == 1 and r == 0:
            mark("wait_small")
            local[1].wait()
            local[3].wait()
            local[4].wait()
            span(me + 1, n_sp, lambda k: send_head(k).wait_send())
        mark(f"stage#n={now}#r={r}#st={st}")
        stage(r, q, st)
        for d, c, k in pieces[:DW_SLOTS.count((r, st))]:
            send_piece(d, c, k).start()
        del pieces[:DW_SLOTS.count((r, st))]

    assert not pieces
    mark("wait_back")
    own_back.wait()
    each(n_sp, me, lambda k: got(ret.at[rows_of(k), :], r_ret.at[k]))
    mark("combine")
    back = ret[...]
    out_ref[...] = (
        stream_s[...]
        + jnp.dot(whi[...], back, preferred_element_type=F32)
        + jnp.dot(wlo[...], back, preferred_element_type=F32)).astype(BF16)

    mark("drain")

    def sent_all(view, sem):
        remote(view, view, sem, sem, me, twin).wait_send()

    sent_all(wx.at[pl.ds(0, n_tp - 1), quarter, :], s_wx)
    sent_all(wx.at[:, pl.ds(0, part * (X_CHIPS - 1)), :], s_wq)
    sent_all(mx.at[pl.ds(0, 2 * n_y - 1)], s_mx)
    sent_all(dw.at[pl.ds(0, n_tp - 1)], s_dw)
    sent_all(xs.at[pl.ds(0, n_sp - 1)], s_dis)
    sent_all(outb.at[pl.ds(0, (n_sp - 1) * cap), :], s_ret)
    for q in range(CHUNKS):
        rows = pl.ds(q * rows_q, rows_q)
        sent_all(g_buf.at[pl.ds(0, 2 * n_y - 1), rows, :], g_sems[0].at[q])
        sent_all(h_buf.at[pl.ds(0, 2 * n_y - 1), rows, :], h_sems[0].at[q])
    mark(None)


def per_device(
    lane_source_signal, spectral_damping_part, spectral_angular_part, interval_exponent,
    entry_matrix_inphase, entry_matrix_quadrature, emission_inphase, emission_quadrature,
    lane_bypass_factor, spike_shrink_offset, lane_exit_matrix, skipline_stream,
    specialist_scaling_vector, selected_specialists, dispatcher_scores,
    specialist_valve_matrix, specialist_widen_matrix, specialist_shrink_matrix,
):
    n_sp, n_tp = lax.axis_size("sp"), lax.axis_size("tp")
    groups, states, lanes = entry_matrix_inphase.shape
    chan, tok = lane_source_signal.shape
    width = specialist_scaling_vector.shape[0]
    d_local = width // n_tp
    f_local = specialist_valve_matrix.shape[2]
    cap = 2 * tok * selected_specialists.shape[1] // n_sp
    slots = n_sp * cap
    dims = (n_sp, n_tp, groups, states, lanes, tok, width, cap)
    vmem = pl.BlockSpec(memory_space=pltpu.VMEM)
    operands = (
        lane_source_signal, spectral_damping_part, spectral_angular_part,
        interval_exponent.reshape(1, groups), entry_matrix_inphase.transpose(0, 2, 1),
        entry_matrix_quadrature.transpose(0, 2, 1),
        emission_inphase, emission_quadrature, lane_bypass_factor.reshape(1, chan),
        spike_shrink_offset, selected_specialists.T, dispatcher_scores.T, lane_exit_matrix,
        skipline_stream, specialist_scaling_vector.reshape(1, width),
        specialist_valve_matrix, specialist_widen_matrix, specialist_shrink_matrix,
    )
    hbm = pl.BlockSpec(memory_space=pl.ANY)
    dma = pltpu.SemaphoreType.DMA
    scratch = [pltpu.VMEM(a.shape, a.dtype) for a in operands[:12]] + [
        pltpu.VMEM((8, 128), F32),
        pltpu.VMEM((n_sp, 8, 128), F32),
        pltpu.VMEM((n_tp, chan, d_local), BF16),
        pltpu.VMEM((n_tp, chan, tok), BF16),
        pltpu.VMEM((n_tp, f_local, d_local), BF16),
        pltpu.VMEM((width, 2 * f_local), BF16),
        pltpu.VMEM((tok, d_local), BF16),
        pltpu.VMEM((1, width), F32),
        pltpu.VMEM((slots, 128), F32),
        pltpu.VMEM((tok, slots), BF16),
        pltpu.VMEM((tok, slots), BF16),
        pltpu.VMEM((tok, slots), BF16),
        pltpu.VMEM((n_sp, cap, d_local), BF16),
        pltpu.VMEM((n_tp, slots, d_local), BF16),
        pltpu.VMEM((n_tp, slots, f_local), BF16),
        pltpu.VMEM((slots, 2 * f_local), F32),
        pltpu.VMEM((slots, d_local), F32),
        pltpu.VMEM((slots, d_local), BF16),
        pltpu.VMEM((slots, d_local), BF16),
        pltpu.VMEM((tok, d_local), F32),
        pltpu.VMEM((groups, lanes, tok), F32),
        pltpu.VMEM((groups, states, tok), F32),
        pltpu.VMEM((groups, states, tok), F32),
        dma((12,)), dma((8,)),
        dma((n_sp,)), dma((n_sp,)),
        dma, dma((n_tp,)), dma, dma((X_CHIPS,)), dma, dma((n_tp,)), dma, dma((n_tp,)),
        dma, dma((n_sp,)), dma, dma((n_sp,)),
    ] + 2 * [
        dma((CHUNKS,)), dma((n_tp, CHUNKS)),
        dma((n_tp // CORES, CHUNKS)), dma((n_tp // CORES, CHUNKS)),
    ]
    return pl.pallas_call(
        functools.partial(mixer_kernel, dims),
        out_shape=pltpu.VMEM((tok, d_local), BF16),
        in_specs=[hbm] * 18,
        out_specs=vmem,
        scratch_shapes=scratch,
        compiler_params=pltpu.CompilerParams(
            collective_id=0, has_side_effects=True, vmem_limit_bytes=60 * 1024 * 1024),
    )(*operands)


def solution(mesh):
    placed = (
        P("tp", "sp"), P("tp", None), P("tp", None), P("tp"), P("tp", None, None),
        P("tp", None, None), P("tp", None, None), P("tp", None, None), P("tp"),
        P("tp", "sp"), P("tp", None), P("sp", None), P(), P("sp", None), P("sp", None),
        P("sp", None, "tp"), P("sp", None, "tp"), P("sp", "tp", None),
    )
    return jax.shard_map(
        per_device, mesh=mesh, in_specs=placed, out_specs=P("sp", "tp"), check_vma=False
    )
```

```python
import functools

import jax
import jax.numpy as jnp
from jax import lax
from jax.experimental import pallas as pl
from jax.experimental.pallas import tpu as pltpu
from jax.sharding import PartitionSpec as P

EPS = 1e-06
HIGH = lax.Precision.HIGHEST
MESH = pl.DeviceIdType.MESH
F32 = jnp.float32
BF16 = jnp.bfloat16
CORES = 2
CHUNKS = 4
SKEW = 0.4
X_CHIPS = 4
DW_EARLY, DW_MID = 4, 12
PIECE = 32
DW_SLOTS = ((2, 3), (3, 3), (0, 4), (1, 4), (2, 4), (3, 4), (0, 6), (1, 6))
GROUP_SETS = ((0, 1, 2, 3),)
CHUNK_ORDER = (0, 1, 2, 3)


def iota(shape, dim):
    return lax.broadcasted_iota(jnp.int32, shape, dim)


def to_col(row):
    n = row.shape[1]
    eye = iota((n, n), 0) == iota((n, n), 1)
    return jnp.sum(jnp.where(eye, row, 0.0), axis=1, keepdims=True)


def to_row(col):
    n = col.shape[0]
    eye = iota((n, n), 0) == iota((n, n), 1)
    return jnp.sum(jnp.where(eye, col, 0.0), axis=0, keepdims=True)


def small_expm1(x):
    total = jnp.ones_like(x)
    for k in range(11, 1, -1):
        total = 1.0 + total * x * (1.0 / k)
    return jnp.where(x > -0.7, x * total, jnp.exp(x) - 1.0)


def dot_first(a, b):
    return lax.dot_general(
        a, b, (((0,), (0,)), ((), ())), precision=HIGH, preferred_element_type=F32)


def times(ar, ai, br, bi):
    return ar * br - ai * bi, ar * bi + ai * br


def mixer_kernel(
    dims,
    u_hbm, damp_hbm, ang_hbm, ie_hbm, ein_hbm, eq_hbm, cin_hbm, cq_hbm, byp_hbm, off_hbm,
    sel_hbm, score_hbm, wexit_hbm, skip_hbm, gain_hbm, gate_hbm, up_hbm, down_hbm,
    out_ref,
    u_ref, damp_ref, ang_ref, ie_ref, ein_ref, eq_ref, cin_ref, cq_ref, byp_ref, off_ref,
    sel_ref, score_ref,
    msg, heads, wx, mx, dw, gu, skip, gain, squares, disp, whi, wlo,
    xs, g_buf, h_buf, acc, oacc, outb, ret, stream_s, loc_r, cum_r, cum_i,
    i_sem, l_sem, s_pre, r_pre, s_wx, r_wx, s_wq, r_wq, s_mx, r_mx, s_dw, r_dw,
    s_dis, r_dis, s_ret, r_ret, *ring_sems,
):
    n_sp, n_tp, groups, states, lanes, tok, width, cap = dims
    n_y = n_tp // CORES
    d_local = width // n_tp
    f_local = gate_hbm.shape[2]
    slots = n_sp * cap
    rows_q = slots // CHUNKS
    sp_q = n_sp // CHUNKS
    me, mt = lax.axis_index("sp"), lax.axis_index("tp")
    y, core = mt // CORES, mt % CORES
    twin = y * CORES + (1 - core)
    x_part = me % X_CHIPS
    away = [k for d in range(1, n_y // 2 + 1) for k in ((d, -d) if 2 * d < n_y else (d,))]

    def chip(k):
        return around(y + k, n_y)

    def around(value, count):
        if count & (count - 1):
            return lax.rem(value + count, count)
        return jnp.bitwise_and(value, count - 1)

    def each(count, mine, fn):
        for j in range(1, count):
            fn(around(mine + j, count))

    n_z = n_sp // X_CHIPS
    near = sorted(
        ((dz, dx) for dz in range(-((n_z - 1) // 2), n_z // 2 + 1)
         for dx in range(-((X_CHIPS - 1) // 2), X_CHIPS // 2 + 1)),
        key=lambda o: (-(abs(o[0]) + abs(o[1])), -abs(o[0]), o))

    def at_offset(dz, dx):
        return around(me // X_CHIPS + dz, n_z) * X_CHIPS + around(x_part + dx, X_CHIPS)

    def place_at(dz, dx):
        back = [
            k for k, (a, b) in enumerate(near)
            if (a + dz) % n_z == 0 and (b + dx) % X_CHIPS == 0]
        return back[0]

    def far_first(fn):
        for dz, dx in near[:-1]:
            fn(dz, dx)

    def span(lo, hi, fn):
        def step(j, carry):
            fn(j)
            return carry
        lax.fori_loop(lo, hi, step, 0)

    def remote(src, dst, send, recv, sp, tp):
        return pltpu.make_async_remote_copy(
            src_ref=src, dst_ref=dst, send_sem=send, recv_sem=recv,
            device_id=(sp, tp), device_id_type=MESH)

    scope = []

    def mark(name):
        if scope:
            scope.pop().__exit__(None, None, None)
        if name:
            scope.append(jax.named_scope(name))
            scope[-1].__enter__()

    heads[...] = jnp.zeros_like(heads)
    barrier = pltpu.get_barrier_semaphore()
    far_first(lambda dz, dx: pl.semaphore_signal(
        barrier, inc=1, device_id=(at_offset(dz, dx), mt), device_id_type=MESH))
    for d in away[::-1]:
        for c in range(CORES):
            pl.semaphore_signal(
                barrier, inc=1, device_id=(me, chip(d) * CORES + c), device_id_type=MESH)
    pl.semaphore_signal(barrier, inc=1, device_id=(me, twin), device_id_type=MESH)

    small = [
        pltpu.make_async_copy(src, dst, i_sem.at[k])
        for k, (src, dst) in enumerate((
            (ie_hbm, ie_ref), (damp_hbm, damp_ref), (ang_hbm, ang_ref), (off_hbm, off_ref),
            (u_hbm, u_ref), (ein_hbm, ein_ref), (eq_hbm, eq_ref), (cin_hbm, cin_ref),
            (cq_hbm, cq_ref), (byp_hbm, byp_ref), (sel_hbm, sel_ref), (score_hbm, score_ref)))
    ]
    for copy in small:
        copy.start()

    mark("local_copies")
    own_cols = pl.ds(pl.multiple_of(mt * d_local, d_local), d_local)
    chan = groups * lanes
    part = chan // X_CHIPS
    quarter = pl.ds(pl.multiple_of(x_part * part, part), part)
    local = [
        pltpu.make_async_copy(skip_hbm.at[:, own_cols], skip, l_sem.at[0]),
        pltpu.make_async_copy(gain_hbm, gain, l_sem.at[1]),
        pltpu.make_async_copy(
            wexit_hbm.at[quarter, own_cols], wx.at[mt, quarter, :], l_sem.at[2]),
        pltpu.make_async_copy(gate_hbm.at[0], gu.at[:, pl.ds(0, f_local)], l_sem.at[3]),
        pltpu.make_async_copy(up_hbm.at[0], gu.at[:, pl.ds(f_local, f_local)], l_sem.at[4]),
        pltpu.make_async_copy(down_hbm.at[0, :, own_cols], dw.at[mt], l_sem.at[5]),
    ]
    for copy in local:
        copy.start()

    mark("state")
    for copy in small:
        copy.wait()
    step_size = jnp.exp(to_col(ie_ref[...]))
    damp, ang = damp_ref[...], ang_ref[...]
    rate, angle = damp * step_size, ang * step_size
    cos, sin = jnp.cos(angle), jnp.sin(angle)
    half = jnp.sin(0.5 * angle)
    num_re = small_expm1(rate) * cos - 2.0 * half * half
    num_im = jnp.exp(rate) * sin
    denom = damp * damp + ang * ang
    fac_re = (num_re * damp + num_im * ang) / denom
    fac_im = (num_im * damp - num_re * ang) / denom
    total = off_ref[...]
    lane_g = iota(total.shape, 1)
    shift = 1
    while shift < tok:
        total = total + jnp.where(lane_g >= shift, pltpu.roll(total, shift, 1), 0.0)
        shift *= 2
    lane = iota((states, tok), 1)
    bypass = byp_ref[...]
    each_group = range(groups)
    rows_g = [slice(g, g + 1) for g in each_group]
    signal = [u_ref[g * lanes:(g + 1) * lanes, :].astype(F32) for g in each_group]
    e_re = [dot_first(ein_ref[g], signal[g]) for g in each_group]
    e_im = [dot_first(eq_ref[g], signal[g]) for g in each_group]
    rate_c = [to_col(rate[row]) for row in rows_g]
    w = [(to_col(cos[row]), to_col(sin[row])) for row in rows_g]
    s = [
        times(to_col(fac_re[row]), to_col(fac_im[row]), e_re[g], e_im[g])
        for g, row in enumerate(rows_g)]
    p = [(jnp.ones((states, tok), F32), jnp.zeros((states, tok), F32))] * groups
    for pair in GROUP_SETS:
        shift = 1
        while shift <= tok:
            taken = (jnp.bitwise_and(lane + 1, shift)) != 0
            for g in pair:
                sums = total[rows_g[g]]
                q_re, q_im = times(*p[g], *w[g])
                p[g] = jnp.where(taken, q_re, p[g][0]), jnp.where(taken, q_im, p[g][1])
                if shift < tok:
                    gap = sums - pltpu.roll(sums, shift, 1)
                    size = jnp.exp(rate_c[g] * float(shift) + jnp.minimum(gap, 0.0))
                    size = jnp.where(lane >= shift, size, 0.0)
                    t_re, t_im = times(
                        *w[g], pltpu.roll(s[g][0], shift, 1), pltpu.roll(s[g][1], shift, 1))
                    s[g] = s[g][0] + size * t_re, s[g][1] + size * t_im
                    w[g] = times(*w[g], *w[g])
            shift *= 2
        for g in pair:
            size = jnp.exp(rate_c[g] * (lane + 1).astype(F32) + total[rows_g[g]])
            cum_r[g], cum_i[g] = size * p[g][0], size * p[g][1]
    last = lane == tok - 1
    for g, row in enumerate(rows_g):
        h_re = to_row(jnp.sum(jnp.where(last, s[g][0], 0.0), axis=1, keepdims=True))
        h_im = to_row(jnp.sum(jnp.where(last, s[g][1], 0.0), axis=1, keepdims=True))
        end = jnp.sum(
            jnp.where(lane_g[row] == tok - 1, total[row], 0.0), axis=1, keepdims=True)
        msg[g:g + 1, 0:states] = h_re
        msg[g:g + 1, states:2 * states] = jnp.broadcast_to(end, (1, states))
        msg[groups + g:groups + g + 1, 0:states] = h_im
        msg[groups + g:groups + g + 1, states:2 * states] = jnp.zeros((1, states), F32)
        loc_r[g] = (
            jnp.dot(cin_ref[g], s[g][0], precision=HIGH, preferred_element_type=F32)
            - jnp.dot(cq_ref[g], s[g][1], precision=HIGH, preferred_element_type=F32)
            + to_col(bypass[:, g * lanes:(g + 1) * lanes]) * signal[g])

    mark("barrier")
    pl.semaphore_wait(barrier, n_sp - 1 + n_tp - 1)

    def send_head(k):
        return remote(msg, heads.at[me], s_pre.at[k], r_pre.at[me], k, mt)

    def head_from(k):
        return remote(msg, heads.at[k], s_pre.at[k], r_pre.at[k], me, mt)

    mark("send_head")
    span(me + 1, n_sp, lambda k: send_head(k).start())

    def columns_of(k):
        return pl.ds(pl.multiple_of(k * d_local, d_local), d_local)

    def send_wx(k):
        return remote(
            wexit_hbm.at[quarter, columns_of(k)], wx.at[mt, quarter, :],
            s_wx, r_wx.at[mt], me, k)

    def quarter_of(j):
        other = (x_part + j) % X_CHIPS
        rows = pl.ds(pl.multiple_of(other * part, part), part)
        return me - x_part + other, wx.at[:, rows, :], other

    def send_quarter(j):
        there, _, _ = quarter_of(j)
        mine = wx.at[:, quarter, :]
        return remote(mine, mine, s_wq, r_wq.at[x_part], there, mt)

    def send_dw(k):
        return remote(
            down_hbm.at[0, :, columns_of(k)], dw.at[mt], s_dw, r_dw.at[mt], me, k)

    def send_piece(d, c, k):
        there = chip(d) * CORES + c
        rows = pl.ds(k * PIECE, PIECE)
        return remote(
            down_hbm.at[0, rows, columns_of(there)], dw.at[mt, rows, :],
            s_dw, r_dw.at[mt], me, there)

    targets = [(d, c) for d in away for c in range(CORES)]

    def send_dw_to(those):
        for d, c in those:
            send_dw(chip(d) * CORES + c).start()

    mark("send_wx")
    each(n_tp, mt, lambda k: send_wx(k).start())
    send_dw_to(targets[:DW_EARLY])

    mark("routing")
    sel, score = sel_ref[...].astype(F32), score_ref[...]
    expert = iota((tok, n_sp), 1).astype(F32)
    hit0 = (to_col(sel[0:1]) == expert).astype(F32)
    hit1 = (to_col(sel[1:2]) == expert).astype(F32)
    hits = (hit0 + hit1).astype(BF16)
    below = (iota((tok, tok), 1) < iota((tok, tok), 0)).astype(F32).astype(BF16)
    rank = jnp.dot(below, hits, preferred_element_type=F32).astype(BF16)
    slot_e, slot_j = iota((n_sp, slots), 0), iota((n_sp, slots), 1)
    spread = ((slot_j >= slot_e * cap) & (slot_j < (slot_e + 1) * cap)).astype(F32).astype(BF16)
    hits_x = jnp.dot(hits, spread, preferred_element_type=F32)
    hit0_x = jnp.dot(hit0.astype(BF16), spread, preferred_element_type=F32)
    rank_x = jnp.dot(rank, spread, preferred_element_type=F32)
    place = jnp.bitwise_and(iota((tok, slots), 1), cap - 1).astype(F32)
    picked = (hits_x > 0.5) & (rank_x == place)
    disp[...] = picked.astype(F32).astype(BF16)
    both = score[0:1] + score[1:2]
    share = jnp.where(hit0_x > 0.5, to_col(score[0:1] / both), to_col(score[1:2] / both))
    share = jnp.where(picked, share, 0.0)
    high = share.astype(BF16)
    whi[...] = high
    wlo[...] = (share - high.astype(F32)).astype(BF16)

    mark("wait_head")
    span(0, me, lambda k: head_from(k).wait_recv())
    mark("enter")
    w_re, w_im = cos, sin
    shift = 1
    while shift < tok:
        w_re, w_im = times(w_re, w_im, w_re, w_im)
        shift *= 2
    in_re, in_im = jnp.zeros_like(rate), jnp.zeros_like(rate)
    for k in range(n_sp - 1):
        head = heads[k]
        size = jnp.exp(rate * float(tok) + head[0:groups, states:2 * states])
        n_re, n_im = times(size * w_re, size * w_im, in_re, in_im)
        n_re = n_re + head[0:groups, 0:states]
        n_im = n_im + head[groups:2 * groups, 0:states]
        in_re = jnp.where(k < me, n_re, in_re)
        in_im = jnp.where(k < me, n_im, in_im)
    for g in range(groups):
        row = slice(g, g + 1)
        c_re, c_im = times(cin_ref[g], cq_ref[g], in_re[row], in_im[row])
        value = (
            loc_r[g]
            + jnp.dot(c_re, cum_r[g], precision=HIGH, preferred_element_type=F32)
            - jnp.dot(c_im, cum_i[g], precision=HIGH, preferred_element_type=F32))
        mx[mt, g * lanes:(g + 1) * lanes, :] = jax.nn.gelu(value).astype(BF16)

    def send_mx(owner, tp):
        return remote(mx.at[owner], mx.at[owner], s_mx, r_mx.at[owner], me, tp)

    mark("send_mx")
    for d in away:
        send_mx(mt, chip(d) * CORES + core).start()
    send_mx(mt, twin).start()

    def got(dst, sem):
        remote(dst, dst, s_mx, sem, me, twin).wait_recv()

    mark("wait_quarter")
    local[2].wait()
    each(n_tp, mt, lambda k: got(wx.at[k, quarter, :], r_wx.at[k]))
    for j in (2, 1, 3):
        send_quarter(j).start()
    send_dw_to(targets[DW_EARLY:DW_MID])
    send_dw(twin).start()

    mark("relay_mx")
    local[0].wait()
    for d in away:
        owner = chip(-d) * CORES + core
        got(mx.at[owner], r_mx.at[owner])
        send_mx(owner, twin).start()
    mark("wait_wq")
    for j in range(1, X_CHIPS):
        _, dst, other = quarter_of(j)
        got(dst, r_wq.at[other])
    mark("wait_mx")
    for d in [0] + away:
        owner = chip(-d) * CORES + (1 - core)
        got(mx.at[owner], r_mx.at[owner])
    mark("project")
    projected = lax.dot_general(
        mx[...].reshape(n_tp * chan, tok), wx[...].reshape(n_tp * chan, d_local),
        (((0,), (0,)), ((), ())), preferred_element_type=F32).astype(BF16)
    stream = (skip[...].astype(F32) + projected.astype(F32)).astype(BF16)
    stream_f = stream.astype(F32)
    stream_s[...] = stream_f

    sent = lax.dot_general(
        disp[...], stream, (((0,), (0,)), ((), ())),
        preferred_element_type=F32).astype(BF16).reshape(n_sp, cap, d_local)
    xs[...] = sent

    def rows_of(k):
        start = k * cap
        return pl.ds(start if isinstance(k, int) else pl.multiple_of(start, cap), cap)

    own_place = n_sp - 1

    def send_rows(dz, dx):
        k, place = at_offset(dz, dx), place_at(dz, dx)
        return remote(
            xs.at[k], g_buf.at[mt, rows_of(place), :], s_dis, r_dis.at[place], k, mt)

    mark("send_rows")
    far_first(lambda dz, dx: send_rows(dz, dx).start())
    own_rows = pltpu.make_async_copy(
        xs.at[me], g_buf.at[mt, rows_of(own_place), :], l_sem.at[6])
    own_rows.start()

    deepest = n_y // 2

    way = 1 - 2 * core
    onward = around(y + way, n_y) * CORES + core

    def rows_in(q):
        return pl.ds(q * rows_q, rows_q)

    def half_in(q, side):
        size = rows_q // CORES
        return pl.ds(pl.multiple_of(q * rows_q + side * size, size), size)

    def chip_rows(buf, there, rows):
        return buf.at[pl.ds(there * CORES, CORES), rows, :]

    def ring_hop(buf, sems, q, h):
        send, one, ring, handed = sems

        def push(view, sem, tp):
            remote(view, view, send.at[q], sem, me, tp).start()

        if h == 0:
            for tp in (chip(1) * CORES, chip(-1) * CORES + 1, twin):
                push(buf.at[mt, rows_in(q), :], one.at[mt, q], tp)
            return
        there = around(y - way * h, n_y)
        view = chip_rows(buf, there, rows_in(q) if h < deepest else half_in(q, core))
        if h == 1:
            for c in range(CORES):
                owner = there * CORES + c
                got(buf.at[owner, rows_in(q), :], one.at[owner, q])
        else:
            got(view, ring.at[there, q])
        if h < deepest:
            rows = rows_in(q) if h < deepest - 1 else half_in(q, core)
            push(chip_rows(buf, there, rows), ring.at[there, q], onward)
        push(view, handed.at[there, q], twin)

    def normed(both, there, rows, fresh):
        depth = CORES * d_local
        full = both.astype(F32)
        square = full * full
        total = square[:, 0:128]
        for k in range(1, depth // 128):
            total = total + square[:, k * 128:(k + 1) * 128]
        squares[rows, :] = total if fresh else squares[rows, :] + total
        gains = gain[:, pl.ds(pl.multiple_of(there * depth, depth), depth)]
        return (full * gains).astype(BF16)

    def pairs(buf, sems, q, h, weights, target, need=None):
        _, one, _, handed = sems
        rows = rows_in(q)

        def multiply(there):
            both = jnp.concatenate(
                [buf[there * CORES, rows, :], buf[there * CORES + 1, rows, :]], axis=1)
            if need is None:
                both = normed(both, there, rows, h == 0)
            part = jnp.dot(both, weights(there), preferred_element_type=F32)
            if h == 0:
                target[rows, :] = part
            else:
                target[rows, :] += part

        if need is not None:
            need(h)
        other = around(y + way * h, n_y)
        if h == 0:
            got(buf.at[twin, rows, :], one.at[twin, q])
        elif h < deepest:
            multiply(around(y - way * h, n_y))
            got(chip_rows(buf, other, rows), handed.at[other, q])
        else:
            got(chip_rows(buf, other, half_in(q, 1 - core)), handed.at[other, q])
        multiply(other)

    def gate_up(there):
        depth = CORES * d_local
        return gu[pl.ds(pl.multiple_of(there * depth, depth), depth), :]

    def down_here(k):
        if k == 0:
            local[5].wait()
            got(dw.at[twin], r_dw.at[twin])
        else:
            for d in (k, -k) if 2 * k < n_y else (k,):
                for c in range(CORES):
                    owner = chip(d) * CORES + c
                    got(dw.at[owner], r_dw.at[owner])

    def down(there):
        return jnp.concatenate([dw[there * CORES], dw[there * CORES + 1]], axis=0)

    def send_back(place):
        k = at_offset(*near[place])
        return remote(
            outb.at[rows_of(place), :], ret.at[rows_of(me), :], s_ret, r_ret.at[me], k, mt)

    own_back = pltpu.make_async_copy(
        outb.at[rows_of(own_place), :], ret.at[rows_of(me), :], l_sem.at[7])

    seen = set()
    g_sems, h_sems = ring_sems[:4], ring_sems[4:]

    def stage(r, q, st):
        rows = slice(q * rows_q, (q + 1) * rows_q)
        first = deepest + 1

        def need(k):
            if k not in seen:
                seen.add(k)
                down_here(k)

        if st == 0:
            for place in range(q * sp_q, (q + 1) * sp_q):
                if place == own_place:
                    own_rows.wait()
                else:
                    got(g_buf.at[mt, rows_of(place), :], r_dis.at[place])
            ring_hop(g_buf, g_sems, q, 0)
        elif st <= deepest:
            ring_hop(g_buf, g_sems, q, st)
            pairs(g_buf, g_sems, q, st - 1, gate_up, acc)
        elif st == first:
            pairs(g_buf, g_sems, q, deepest, gate_up, acc)
            mean = jnp.sum(squares[rows, :], axis=1, keepdims=True) * (1.0 / width)
            factor = lax.rsqrt(mean + EPS)
            gate = acc[rows, 0:f_local] * factor
            wide = acc[rows, f_local:2 * f_local] * factor
            h_buf[mt, rows, :] = (jax.nn.silu(gate) * wide).astype(BF16)
            ring_hop(h_buf, h_sems, q, 0)
        elif st <= first + deepest:
            ring_hop(h_buf, h_sems, q, st - first)
            pairs(h_buf, h_sems, q, st - first - 1, down, oacc, need)
        else:
            pairs(h_buf, h_sems, q, deepest, down, oacc, need)
            outb[rows, :] = oacc[rows, :].astype(BF16)

            for place in range(q * sp_q, (q + 1) * sp_q):
                if place == own_place:
                    own_back.start()
                else:
                    send_back(place).start()

    last_stage = 2 * deepest + 2
    pieces = [
        (d, c, k) for d, c in targets[DW_MID:] for k in range(f_local // PIECE)]
    order = sorted(
        (st + SKEW * r if st else -1, r, q, st)
        for r, q in enumerate(CHUNK_ORDER) for st in range(last_stage + 1))
    for now, (_, r, q, st) in enumerate(order):
        if st == 1 and r == 0:
            mark("wait_small")
            local[1].wait()
            local[3].wait()
            local[4].wait()
            span(me + 1, n_sp, lambda k: send_head(k).wait_send())
        mark(f"stage#n={now}#r={r}#st={st}")
        stage(r, q, st)
        for d, c, k in pieces[:DW_SLOTS.count((r, st))]:
            send_piece(d, c, k).start()
        del pieces[:DW_SLOTS.count((r, st))]

    assert not pieces
    mark("wait_back")
    own_back.wait()
    each(n_sp, me, lambda k: got(ret.at[rows_of(k), :], r_ret.at[k]))
    mark("combine")
    back = ret[...]
    out_ref[...] = (
        stream_s[...]
        + jnp.dot(whi[...], back, preferred_element_type=F32)
        + jnp.dot(wlo[...], back, preferred_element_type=F32)).astype(BF16)

    mark("drain")

    def sent_all(view, sem):
        remote(view, view, sem, sem, me, twin).wait_send()

    sent_all(wx.at[pl.ds(0, n_tp - 1), quarter, :], s_wx)
    sent_all(wx.at[:, pl.ds(0, part * (X_CHIPS - 1)), :], s_wq)
    sent_all(mx.at[pl.ds(0, 2 * n_y - 1)], s_mx)
    sent_all(dw.at[pl.ds(0, n_tp - 1)], s_dw)
    sent_all(xs.at[pl.ds(0, n_sp - 1)], s_dis)
    sent_all(outb.at[pl.ds(0, (n_sp - 1) * cap), :], s_ret)
    for q in range(CHUNKS):
        rows = pl.ds(q * rows_q, rows_q)
        sent_all(g_buf.at[pl.ds(0, 2 * n_y - 1), rows, :], g_sems[0].at[q])
        sent_all(h_buf.at[pl.ds(0, 2 * n_y - 1), rows, :], h_sems[0].at[q])
    mark(None)


def per_device(
    lane_source_signal, spectral_damping_part, spectral_angular_part, interval_exponent,
    entry_matrix_inphase, entry_matrix_quadrature, emission_inphase, emission_quadrature,
    lane_bypass_factor, spike_shrink_offset, lane_exit_matrix, skipline_stream,
    specialist_scaling_vector, selected_specialists, dispatcher_scores,
    specialist_valve_matrix, specialist_widen_matrix, specialist_shrink_matrix,
):
    n_sp, n_tp = lax.axis_size("sp"), lax.axis_size("tp")
    groups, states, lanes = entry_matrix_inphase.shape
    chan, tok = lane_source_signal.shape
    width = specialist_scaling_vector.shape[0]
    d_local = width // n_tp
    f_local = specialist_valve_matrix.shape[2]
    cap = 2 * tok * selected_specialists.shape[1] // n_sp
    slots = n_sp * cap
    dims = (n_sp, n_tp, groups, states, lanes, tok, width, cap)
    vmem = pl.BlockSpec(memory_space=pltpu.VMEM)
    operands = (
        lane_source_signal, spectral_damping_part, spectral_angular_part,
        interval_exponent.reshape(1, groups), entry_matrix_inphase.transpose(0, 2, 1),
        entry_matrix_quadrature.transpose(0, 2, 1),
        emission_inphase, emission_quadrature, lane_bypass_factor.reshape(1, chan),
        spike_shrink_offset, selected_specialists.T, dispatcher_scores.T, lane_exit_matrix,
        skipline_stream, specialist_scaling_vector.reshape(1, width),
        specialist_valve_matrix, specialist_widen_matrix, specialist_shrink_matrix,
    )
    hbm = pl.BlockSpec(memory_space=pl.ANY)
    dma = pltpu.SemaphoreType.DMA
    scratch = [pltpu.VMEM(a.shape, a.dtype) for a in operands[:12]] + [
        pltpu.VMEM((8, 128), F32),
        pltpu.VMEM((n_sp, 8, 128), F32),
        pltpu.VMEM((n_tp, chan, d_local), BF16),
        pltpu.VMEM((n_tp, chan, tok), BF16),
        pltpu.VMEM((n_tp, f_local, d_local), BF16),
        pltpu.VMEM((width, 2 * f_local), BF16),
        pltpu.VMEM((tok, d_local), BF16),
        pltpu.VMEM((1, width), F32),
        pltpu.VMEM((slots, 128), F32),
        pltpu.VMEM((tok, slots), BF16),
        pltpu.VMEM((tok, slots), BF16),
        pltpu.VMEM((tok, slots), BF16),
        pltpu.VMEM((n_sp, cap, d_local), BF16),
        pltpu.VMEM((n_tp, slots, d_local), BF16),
        pltpu.VMEM((n_tp, slots, f_local), BF16),
        pltpu.VMEM((slots, 2 * f_local), F32),
        pltpu.VMEM((slots, d_local), F32),
        pltpu.VMEM((slots, d_local), BF16),
        pltpu.VMEM((slots, d_local), BF16),
        pltpu.VMEM((tok, d_local), F32),
        pltpu.VMEM((groups, lanes, tok), F32),
        pltpu.VMEM((groups, states, tok), F32),
        pltpu.VMEM((groups, states, tok), F32),
        dma((12,)), dma((8,)),
        dma((n_sp,)), dma((n_sp,)),
        dma, dma((n_tp,)), dma, dma((X_CHIPS,)), dma, dma((n_tp,)), dma, dma((n_tp,)),
        dma, dma((n_sp,)), dma, dma((n_sp,)),
    ] + 2 * [
        dma((CHUNKS,)), dma((n_tp, CHUNKS)),
        dma((n_tp // CORES, CHUNKS)), dma((n_tp // CORES, CHUNKS)),
    ]
    return pl.pallas_call(
        functools.partial(mixer_kernel, dims),
        out_shape=pltpu.VMEM((tok, d_local), BF16),
        in_specs=[hbm] * 18,
        out_specs=vmem,
        scratch_shapes=scratch,
        compiler_params=pltpu.CompilerParams(
            collective_id=0, has_side_effects=True, vmem_limit_bytes=60 * 1024 * 1024),
    )(*operands)


def solution(mesh):
    placed = (
        P("tp", "sp"), P("tp", None), P("tp", None), P("tp"), P("tp", None, None),
        P("tp", None, None), P("tp", None, None), P("tp", None, None), P("tp"),
        P("tp", "sp"), P("tp", None), P("sp", None), P(), P("sp", None), P("sp", None),
        P("sp", None, "tp"), P("sp", None, "tp"), P("sp", "tp", None),
    )
    return jax.shard_map(
        per_device, mesh=mesh, in_specs=placed, out_specs=P("sp", "tp"), check_vma=False
    )
```
